32 devices in a mesh: sp: 8 (over z, core), tp: 4 (over y, x).
Axes of the slice: x: 2, y: 2, z: 4, core: 2. Of those that a mesh axis runs over, the one named last changes fastest.
Arguments:
- resid: bfloat16 [2048, 2048], P('sp'), may hold values from -18 to 18
- narrow_head_input: bfloat16 [2048, 1024], P('sp', 'tp'), may hold values from -6 to 6
- wide_head_input: bfloat16 [2048, 2048], P('sp', 'tp'), may hold values from -6 to 6
- key_group_input: bfloat16 [2048, 512], P('sp'), may hold values from -6 to 6
- query_group_input: bfloat16 [2048, 512], P('sp'), may hold values from -6 to 6
- narrow_output_gate: bfloat16 [2048, 1024], P('sp', 'tp'), may hold values from -6 to 6
- wide_output_gate: bfloat16 [2048, 2048], P('sp', 'tp'), may hold values from -6 to 6
- step_input_rows: bfloat16 [2048, 2, 16], P('sp', None, 'tp'), may hold values from -4 to 4
- head_decay_logarithm: float32 [2, 16], P(None, 'tp'), may hold values from -14 to -2
- position_log_decay: float32 [2048, 2, 16], P('sp', None, 'tp'), may hold values from -1.4 to 0
- direct_input_weight: float32 [2, 16], P(None, 'tp'), may hold values from 0.5 to 2
- narrow_conv_taps: float32 [4, 1024], P(None, 'tp'), may hold values from -3 to 3
- wide_conv_taps: float32 [4, 2048], P(None, 'tp'), may hold values from -3 to 3
- key_conv_taps: float32 [4, 512], replicated, may hold values from -3 to 3
- query_conv_taps: float32 [4, 512], replicated, may hold values from -3 to 3
- narrow_norm_gain: float32 [1024], P('tp'), may hold values from 0.1 to 1.9
- wide_norm_gain: float32 [2048], P('tp'), may hold values from 0.1 to 1.9
- narrow_output_rows: bfloat16 [1024, 2048], P('tp'), may hold values from -0.109375 to 0.109375
- wide_output_rows: bfloat16 [2048, 2048], P('tp'), may hold values from -0.109375 to 0.109375
- feedforward_norm_gain: float32 [2048], replicated, may hold values from 0.1 to 1.9
- routes: int32 [2048, 3], P('sp'), may hold values from 0 to 7, all different within a row; in each aligned block of 256 rows (0 to 255, 256 to 511, ...) at most 128 rows name the same one
- routing_weight_values: float32 [2048, 3], P('sp'), may hold values from 0.1 to 1
- expert_gate_matrix: bfloat16 [8, 2048, 2048], P('sp', None, 'tp'), may hold values from -1 to 1
- expert_up_matrix: bfloat16 [8, 2048, 2048], P('sp', None, 'tp'), may hold values from -1 to 1
- expert_down_matrix: bfloat16 [8, 2048, 2048], P('sp', 'tp'), may hold values from -0.015625 to 0.015625
Outputs:
- layer_out: bfloat16 [2048, 2048], P('sp', 'tp')
The draws below stay inside these ranges and needn't reach their ends.
Inputs may be any that keep to these rules, and one draw needn't show every extreme that they name: `routes`: each token names 3 different experts. Among the tokens of one index of sp (aligned blocks of 256 rows) no expert is named by more than 128 of them, and in some blocks one is named by exactly 128.
All inputs are finite; a program needn't handle non-finite values.
Results may differ from the reference program's by a relative error of at most 0.015.
Values may be sent and summed in bfloat16 or wider, within the bound.
A program may use at most 64 MiB of HBM per device.

```python
import math
import jax
import jax.numpy as jnp
import numpy as np
from jax import lax

D = 2048
HEADS = 16
NARROW_HEAD_DIM = 64
WIDE_HEAD_DIM = 128
STATE = 128
GROUPS = 4
CONV_W = 4
BLOCK = 128
FF = 2048
TOPK = 3
TOK_SP = 256
TOKENS = 2048
EXPERTS = 8
CAP = 128
N_SP = 8
N_TP = 4


def draw_resid(key, part):
    key_base, key_rows = jax.random.split(jax.random.fold_in(key, 3), 2)
    row_scales = jnp.exp(jax.random.uniform(key_rows, (TOKENS, 1), jnp.float32, math.log(0.3), math.log(3.0)))
    base = jnp.clip(jax.random.normal(key_base, (TOKENS, D), jnp.float32), -6.0, 6.0)
    return jnp.clip(base * row_scales, -18.0, 18.0).astype(jnp.bfloat16)


def draw_step_input_rows(key, part):
    key_base, key_shift = jax.random.split(jax.random.fold_in(key, 5))
    block_total = TOKENS // TOK_SP
    shifts = jax.random.uniform(key_shift, (block_total, 1, 1, 1), jnp.float32, -1.0, 1.0)
    base = jax.random.normal(key_base, (block_total, TOK_SP, 2, HEADS), jnp.float32)
    return jnp.clip(base + shifts, -4.0, 4.0).reshape(TOKENS, 2, HEADS).astype(jnp.bfloat16)


def draw_head_decay_logarithm(key, part):
    key_kind, key_slow, key_fast = jax.random.split(jax.random.fold_in(key, 7), 3)
    slow_share = 0.5
    slow_heads = jax.random.uniform(key_kind, (2, HEADS), jnp.float32) < slow_share
    slow_rate = jnp.exp(jax.random.uniform(key_slow, (2, HEADS), jnp.float32, math.log(0.1), math.log(0.6))) / TOKENS
    fast_rate = jnp.exp(jax.random.uniform(key_fast, (2, HEADS), jnp.float32, math.log(1.0 / 60.0), math.log(1.0 / 20.0)))
    return jnp.clip(jnp.log(jnp.where(slow_heads, slow_rate, fast_rate)), -14.0, -2.0).astype(jnp.float32)


def draw_position_log_decay(key, part):
    key_spots, key_depth = jax.random.split(jax.random.fold_in(key, 9))
    spots = jax.random.randint(key_spots, (3,), 0, TOKENS)
    depth = jax.random.uniform(key_depth, (3, 2, HEADS), jnp.float32, math.log(0.5), math.log(0.8))
    hits = (jnp.arange(TOKENS)[:, None] == spots[None, :]).astype(jnp.float32)
    return jnp.clip(jnp.einsum('tk,khd->thd', hits, depth), -1.4, 0.0).astype(jnp.float32)


def draw_expert_gate_matrix(key, part):
    key_base, key_cols = jax.random.split(jax.random.fold_in(key, 11))
    column_scales = jnp.exp(jax.random.uniform(key_cols, (EXPERTS, 1, FF), jnp.float32, math.log(0.5), math.log(8.0)))
    base = jax.random.normal(key_base, (EXPERTS, D, FF), jnp.float32)
    return jnp.clip(base * column_scales / math.sqrt(D), -1.0, 1.0).astype(jnp.bfloat16)


def draw_expert_up_matrix(key, part):
    key_base, key_cols = jax.random.split(jax.random.fold_in(key, 13))
    column_scales = jnp.exp(jax.random.uniform(key_cols, (EXPERTS, 1, FF), jnp.float32, math.log(0.5), math.log(8.0)))
    base = jax.random.normal(key_base, (EXPERTS, D, FF), jnp.float32)
    return jnp.clip(base * column_scales / math.sqrt(D), -1.0, 1.0).astype(jnp.bfloat16)


def level_of(own_key, dims, shards, least, high):
    def one(dim, blocks):
        draws = jax.random.uniform(jax.random.fold_in(jax.random.fold_in(own_key, 6), dim), (blocks,), jnp.float32, least / len(shards), high / len(shards))
        return jnp.repeat(jnp.exp(draws), dims[dim] // blocks).reshape((-1,) + (1,) * (len(dims) - dim - 1))

    gain = one(*shards[0])
    for cut in shards[1:]:
        gain = gain * one(*cut)
    return gain


def shared_out(rng, own, number, rows, amount, top, limit, lean):
    sequence = jax.random.permutation(rng, amount)
    crowded, common = portions_of(amount, rows * top, limit, lean, True), portions_of(amount, rows * top, limit, lean, False)
    places = jnp.arange(amount)

    def named(tallies, offset_by):
        used = int((tallies > 0).sum())
        fixed = max(1, used // 4)
        moved = fixed + (places - fixed + offset_by * (used - fixed)) % max(1, amount - fixed)
        return jnp.zeros((amount,), jnp.int32).at[sequence[jnp.where(places < fixed, places, moved)]].set(jnp.asarray(tallies, jnp.int32))

    tallies = jnp.where(number % 4 == 0, named(crowded, number // 4), named(common, number - number // 4 - 1))
    mixed = jax.random.permutation(jax.random.fold_in(own, 3), amount)
    giver, sink = mixed[0:amount // 2 * 2:2], mixed[1:amount // 2 * 2:2]
    margin = jnp.minimum(tallies[giver] - 1, limit - tallies[sink]) // 2
    margin = jnp.where((giver == sequence[0]) | (sink == sequence[0]) | (tallies[sink] == 0), 0, jnp.maximum(margin, 0))
    moved = jax.random.randint(jax.random.fold_in(own, 4), (amount // 2,), 0, 1 << 20) % (margin + 1)
    tallies = tallies.at[giver].add(-moved).at[sink].add(moved)
    members = jnp.searchsorted(jnp.cumsum(tallies), jnp.arange(rows * top), side="right").astype(jnp.int32)
    listing = members.reshape(top, rows).T
    listing = listing[jax.random.permutation(jax.random.fold_in(own, 1), rows)]
    offset_by = jax.random.randint(jax.random.fold_in(own, 2), (rows, 1), 0, top)
    return jnp.take_along_axis(listing, (jnp.arange(top)[None, :] + offset_by) % top, axis=1)


def portions_of(number_of, total, bound, lean, full):
    portions = [(1 << 20) // math.isqrt(standing ** lean) + 1 for standing in range(1, number_of + 1)]
    largest = bound if full else min(bound, max(-(-total // number_of), total * portions[0] // sum(portions)))
    least = 1 if total - largest >= number_of - 1 else 0
    holding, surplus = [largest] + [least] * (number_of - 1), total - largest - least * (number_of - 1)
    while surplus > 0:
        movable = [i for i in range(1, number_of) if holding[i] < largest] or [i for i in range(1, number_of) if holding[i] < bound]
        pool, left = sum([portions[i] for i in movable]), surplus
        for i in movable:
            extra = min(bound - holding[i], max(1, left * portions[i] // pool), surplus)
            holding[i] = holding[i] + extra
            surplus = surplus - extra
    return np.array(holding)


def normal_values(rng, shape, deviation, limit, cuts=(), kind=jnp.bfloat16):
    drawn = deviation * jax.random.normal(rng, shape, jnp.float32)
    if cuts:
        drawn = drawn * level_of(rng, shape, cuts, -0.22, 0.18)
    return jnp.clip(drawn, -limit, limit).astype(kind)


def setup_inputs(seed: int = 0) -> dict:
    splits = jax.random.split(jax.random.key(seed), 26)
    resid = draw_resid(jax.random.fold_in(splits[25], 71), 0)
    narrow_head_input = normal_values(splits[1], (TOKENS, HEADS * NARROW_HEAD_DIM), 1.0, 6.0, ((0, 8), (1, 4)))
    wide_head_input = normal_values(splits[2], (TOKENS, HEADS * WIDE_HEAD_DIM), 1.0, 6.0, ((0, 8), (1, 4)))
    key_group_input = normal_values(splits[3], (TOKENS, GROUPS * STATE), 1.0, 6.0, ((0, 8),))
    query_group_input = normal_values(splits[4], (TOKENS, GROUPS * STATE), 1.0, 6.0, ((0, 8),))
    narrow_output_gate = normal_values(splits[5], (TOKENS, HEADS * NARROW_HEAD_DIM), 1.0, 6.0, ((0, 8), (1, 4)))
    wide_output_gate = normal_values(splits[6], (TOKENS, HEADS * WIDE_HEAD_DIM), 1.0, 6.0, ((0, 8), (1, 4)))
    step_input_rows = draw_step_input_rows(jax.random.fold_in(splits[25], 71), 0)
    head_decay_logarithm = draw_head_decay_logarithm(jax.random.fold_in(splits[25], 71), 0)
    position_log_decay = draw_position_log_decay(jax.random.fold_in(splits[25], 71), 0)
    direct_input_weight = jnp.clip(0.5 + 1.5 * jax.random.uniform(splits[10], (2, HEADS), jnp.float32) ** level_of(splits[10], (2, HEADS), ((1, 4),), -0.2, 0.2), 0.5, 2.0)
    narrow_conv_taps = normal_values(splits[11], (CONV_W, HEADS * NARROW_HEAD_DIM), CONV_W ** -0.5, 3.0, ((1, 4),), jnp.float32)
    wide_conv_taps = normal_values(splits[12], (CONV_W, HEADS * WIDE_HEAD_DIM), CONV_W ** -0.5, 3.0, ((1, 4),), jnp.float32)
    key_conv_taps = normal_values(splits[13], (CONV_W, GROUPS * STATE), CONV_W ** -0.5, 3.0, (), jnp.float32)
    query_conv_taps = normal_values(splits[14], (CONV_W, GROUPS * STATE), CONV_W ** -0.5, 3.0, (), jnp.float32)
    narrow_norm_gain = jnp.clip(1.0 + 0.18 * jax.random.normal(splits[15], (HEADS * NARROW_HEAD_DIM,), jnp.float32), 0.1, 1.9)
    wide_norm_gain = jnp.clip(1.0 + 0.18 * jax.random.normal(splits[16], (HEADS * WIDE_HEAD_DIM,), jnp.float32), 0.1, 1.9)
    narrow_output_rows = normal_values(splits[17], (HEADS * NARROW_HEAD_DIM, D), (HEADS * (NARROW_HEAD_DIM + WIDE_HEAD_DIM)) ** -0.5, 0.109375, ((0, 4),))
    wide_output_rows = normal_values(splits[18], (HEADS * WIDE_HEAD_DIM, D), (HEADS * (NARROW_HEAD_DIM + WIDE_HEAD_DIM)) ** -0.5, 0.109375, ((0, 4),))
    feedforward_norm_gain = jnp.clip(1.0 + 0.18 * jax.random.normal(splits[19], (D,), jnp.float32), 0.1, 1.9)
    routes_keys = jax.random.split(jax.random.fold_in(splits[20], 1), TOKENS // TOK_SP)
    routes_turns = jax.random.permutation(jax.random.fold_in(splits[20], 3), TOKENS // TOK_SP)
    routes = jax.vmap(lambda own, number: shared_out(jax.random.fold_in(splits[20], 2), own, number, TOK_SP, EXPERTS, TOPK, CAP, 1))(routes_keys, routes_turns).reshape((TOKENS, TOPK))
    routing_weight_values = jnp.clip(0.1 + 0.9 * jax.random.uniform(splits[21], (TOKENS, TOPK), jnp.float32) ** level_of(splits[21], (TOKENS, TOPK), ((0, 8),), -0.2, 0.2), 0.1, 1.0)
    expert_gate_matrix = draw_expert_gate_matrix(jax.random.fold_in(splits[25], 71), 0)
    expert_up_matrix = draw_expert_up_matrix(jax.random.fold_in(splits[25], 71), 0)
    expert_down_matrix = normal_values(splits[24], (EXPERTS, FF, D), (64 * FF) ** -0.5, 0.015625, ((0, 8), (1, 4)))
    return {"resid": resid, "narrow_head_input": narrow_head_input, "wide_head_input": wide_head_input, "key_group_input": key_group_input, "query_group_input": query_group_input, "narrow_output_gate": narrow_output_gate, "wide_output_gate": wide_output_gate, "step_input_rows": step_input_rows, "head_decay_logarithm": head_decay_logarithm, "position_log_decay": position_log_decay, "direct_input_weight": direct_input_weight, "narrow_conv_taps": narrow_conv_taps, "wide_conv_taps": wide_conv_taps, "key_conv_taps": key_conv_taps, "query_conv_taps": query_conv_taps, "narrow_norm_gain": narrow_norm_gain, "wide_norm_gain": wide_norm_gain, "narrow_output_rows": narrow_output_rows, "wide_output_rows": wide_output_rows, "feedforward_norm_gain": feedforward_norm_gain, "routes": routes, "routing_weight_values": routing_weight_values, "expert_gate_matrix": expert_gate_matrix, "expert_up_matrix": expert_up_matrix, "expert_down_matrix": expert_down_matrix}


NORM_EPS = 1e-06
CLAMP_LIMIT = 7.0
SIGMOID_SCALE = 1.702
FULL_PRECISION = lax.Precision.HIGHEST

def conv_with_rim(values, rim_rows, weight):
    length = values.shape[0]
    padded = jnp.concatenate([rim_rows, values], axis=0).astype(jnp.float32)
    accumulated = jnp.zeros((length, values.shape[1]), jnp.float32)
    for tap_index in range(weight.shape[0]):
        accumulated = accumulated + weight[tap_index] * padded[tap_index:tap_index + length]
    return jax.nn.silu(accumulated)

def pick_groups(channel_table, first_head, head_count):
    length = channel_table.shape[0]
    grouped = channel_table.reshape(length, GROUPS, -1)
    owners = (first_head + jnp.arange(head_count, dtype=jnp.int32)) // (HEADS // GROUPS)
    chooser = (owners[:, None] == jnp.arange(GROUPS, dtype=jnp.int32)[None, :]).astype(jnp.float32)
    return jnp.einsum('sgn,hg->shn', grouped, chooser, precision=FULL_PRECISION)

def local_head(values, step_logarithm, key_head_rows, query_head_rows, block_len):
    block_count = values.shape[0] // block_len
    values = values.reshape(block_count, block_len, -1)
    step_logarithm = step_logarithm.reshape(block_count, block_len)
    key_head_rows = key_head_rows.reshape(block_count, block_len, -1)
    query_head_rows = query_head_rows.reshape(block_count, block_len, -1)
    cum_decay = jnp.cumsum(step_logarithm, axis=1)
    causal_mask = jnp.arange(block_len)[:, None] >= jnp.arange(block_len)[None, :]
    decay_gaps = jnp.where(causal_mask[None], cum_decay[:, :, None] - cum_decay[:, None, :], -1e+30)
    scores = jnp.einsum('bln,bsn->bls', query_head_rows, key_head_rows, precision=FULL_PRECISION) * jnp.exp(decay_gaps)
    inside = jnp.einsum('bls,bsp->blp', scores, values, precision=FULL_PRECISION)
    tail_decay = jnp.exp(cum_decay[:, -1:] - cum_decay)
    states = jnp.einsum('bln,blp->bnp', key_head_rows * tail_decay[..., None], values, precision=FULL_PRECISION)
    totals = cum_decay[:, -1]

    def walk(running, member):
        return (jnp.exp(member[1]) * running + member[0], running)
    closing, entering = lax.scan(walk, jnp.zeros(states.shape[1:], jnp.float32), (states, totals))
    before = jnp.cumsum(totals) - totals
    return (inside, entering, closing, jnp.sum(totals), before, cum_decay, query_head_rows)

def finish_head(inside, entering, before, cum_decay, query_blocks, carried):
    starting = entering + jnp.exp(before)[:, None, None] * carried[None]
    readout = jnp.einsum('bln,bnp->blp', query_blocks * jnp.exp(cum_decay)[..., None], starting, precision=FULL_PRECISION)
    return (inside + readout).reshape(-1, inside.shape[-1])

def group_out(scanned, mixed_input_rows, direct_input_term, gate_input_rows, norm_gain_vector):
    length, head_count, head_dimension = mixed_input_rows.shape
    gated = jax.nn.silu(gate_input_rows.astype(jnp.float32)).reshape(length, head_count, head_dimension)
    result = (scanned + direct_input_term[None, :, None] * mixed_input_rows) * gated
    result = result * lax.rsqrt(lax.optimization_barrier(jnp.mean(result * result, axis=-1, keepdims=True)) + NORM_EPS)
    return (result.reshape(length, head_count * head_dimension) * norm_gain_vector).astype(jnp.bfloat16)

def mixer_head_group(unprojected_input, gate_input_rows, convolution_weight, key_head_table, query_head_table, unsoftened_step, decay_vector, position_decay_rows, direct_input_term, norm_gain_vector, head_dimension):
    length = unprojected_input.shape[0]
    zero_rim = jnp.zeros((convolution_weight.shape[0] - 1, unprojected_input.shape[1]), unprojected_input.dtype)
    mixed_input_rows = conv_with_rim(unprojected_input, zero_rim, convolution_weight).reshape(length, -1, head_dimension)
    head_count = mixed_input_rows.shape[1]
    key_head_rows = pick_groups(key_head_table, 0, head_count)
    query_head_rows = pick_groups(query_head_table, 0, head_count)
    step_length_values = jax.nn.softplus(unsoftened_step.astype(jnp.float32))
    step_logarithm = -jnp.exp(decay_vector)[None, :] * step_length_values + position_decay_rows
    values = mixed_input_rows * step_length_values[..., None]

    def one_head(head_values, head_log, head_keys, head_queries):
        parts = local_head(head_values, head_log, head_keys, head_queries, BLOCK)
        return finish_head(parts[0], parts[1], parts[4], parts[5], parts[6], jnp.zeros_like(parts[2]))
    scanned = jax.vmap(one_head, in_axes=(1, 1, 1, 1), out_axes=1)(values, step_logarithm, key_head_rows, query_head_rows)
    return group_out(scanned, mixed_input_rows, direct_input_term, gate_input_rows, norm_gain_vector)

def expert_layer(normed, routes, expert_gate_matrix, expert_up_matrix, expert_down_matrix):
    tokens = normed.shape[0]
    flat_routes = routes.reshape(-1).astype(jnp.int32)
    order_ids = jnp.argsort(flat_routes, stable=True).astype(jnp.int32)
    sorted_routes = flat_routes[order_ids]
    counts = lax.optimization_barrier(jnp.sum((flat_routes[:, None] == jnp.arange(EXPERTS, dtype=jnp.int32)[None, :]).astype(jnp.int32), axis=0))
    starts = (jnp.cumsum(counts) - counts).astype(jnp.int32)
    room = CAP * N_SP
    padded_ids = jnp.concatenate([order_ids, jnp.zeros((room,), jnp.int32)])

    def one_expert(member):
        start, gate_weight, up_weight, down_weight = member
        picked = lax.dynamic_slice_in_dim(padded_ids, start, room)
        rows = normed[picked // TOPK]
        gate_pre = jnp.dot(rows, gate_weight, preferred_element_type=jnp.float32)
        up_pre = jnp.dot(rows, up_weight, preferred_element_type=jnp.float32)
        clamped = jnp.minimum(gate_pre, CLAMP_LIMIT)
        act = ((jnp.clip(up_pre, -CLAMP_LIMIT, CLAMP_LIMIT) + 1.0) * clamped * jax.nn.sigmoid(SIGMOID_SCALE * clamped)).astype(jnp.bfloat16)
        pieces = act.reshape(room, N_TP, -1).astype(jnp.float32)
        blocks = down_weight.reshape(N_TP, -1, down_weight.shape[1]).astype(jnp.float32)
        partials = jnp.einsum('rtf,tfd->rtd', pieces, blocks)
        rounded = lax.optimization_barrier(partials.astype(jnp.bfloat16)).astype(jnp.float32)
        return lax.optimization_barrier(jnp.sum(rounded, axis=1)).astype(jnp.bfloat16)
    outputs = lax.map(one_expert, (starts, expert_gate_matrix, expert_up_matrix, expert_down_matrix))
    within = jnp.arange(tokens * TOPK, dtype=jnp.int32) - starts[sorted_routes]
    per_sorted = outputs.reshape(EXPERTS * room, -1)[sorted_routes * room + within]
    per_entry = jnp.zeros((tokens * TOPK, per_sorted.shape[1]), jnp.bfloat16).at[order_ids].set(per_sorted)
    return per_entry.reshape(tokens, TOPK, -1)

def reference(resid, narrow_head_input, wide_head_input, key_group_input, query_group_input, narrow_output_gate, wide_output_gate, step_input_rows, head_decay_logarithm, position_log_decay, direct_input_weight, narrow_conv_taps, wide_conv_taps, key_conv_taps, query_conv_taps, narrow_norm_gain, wide_norm_gain, narrow_output_rows, wide_output_rows, feedforward_norm_gain, routes, routing_weight_values, expert_gate_matrix, expert_up_matrix, expert_down_matrix):
    length = resid.shape[0]
    zero_rim = jnp.zeros((CONV_W - 1, key_group_input.shape[1]), key_group_input.dtype)
    key_head_table = conv_with_rim(key_group_input, zero_rim, key_conv_taps)
    query_head_table = conv_with_rim(query_group_input, zero_rim, query_conv_taps)
    narrow_head_output = mixer_head_group(narrow_head_input, narrow_output_gate, narrow_conv_taps, key_head_table, query_head_table, step_input_rows[:, 0], head_decay_logarithm[0], position_log_decay[:, 0], direct_input_weight[0], narrow_norm_gain, NARROW_HEAD_DIM)
    wide_head_output = mixer_head_group(wide_head_input, wide_output_gate, wide_conv_taps, key_head_table, query_head_table, step_input_rows[:, 1], head_decay_logarithm[1], position_log_decay[:, 1], direct_input_weight[1], wide_norm_gain, WIDE_HEAD_DIM)
    narrow_blocks = narrow_head_output.reshape(length, N_TP, -1).transpose(1, 0, 2)
    wide_blocks = wide_head_output.reshape(length, N_TP, -1).transpose(1, 0, 2)
    narrow_weights = narrow_output_rows.reshape(N_TP, -1, narrow_output_rows.shape[1])
    wide_weights = wide_output_rows.reshape(N_TP, -1, wide_output_rows.shape[1])

    def project(running, member):
        part_narrow, part_wide, weight_narrow, weight_wide = member
        term = jnp.dot(part_narrow, weight_narrow, preferred_element_type=jnp.float32)
        term = term + jnp.dot(part_wide, weight_wide, preferred_element_type=jnp.float32)
        return (running + lax.optimization_barrier(term.astype(jnp.bfloat16)).astype(jnp.float32), None)
    mixed, _ = lax.scan(project, jnp.zeros((length, narrow_output_rows.shape[1]), jnp.float32), (narrow_blocks, wide_blocks, narrow_weights, wide_weights))
    hidden_state = resid.astype(jnp.float32) + mixed
    normed = (hidden_state * lax.rsqrt(lax.optimization_barrier(jnp.mean(hidden_state * hidden_state, axis=-1, keepdims=True)) + NORM_EPS) * feedforward_norm_gain).astype(jnp.bfloat16)
    expert_rows = expert_layer(normed, routes, expert_gate_matrix, expert_up_matrix, expert_down_matrix)
    combined = lax.optimization_barrier(jnp.sum(expert_rows.astype(jnp.float32) * routing_weight_values[..., None], axis=1))
    return (hidden_state + combined).astype(jnp.bfloat16)
```

```python
import functools

import jax
import jax.numpy as jnp
from jax import lax
from jax.experimental import pallas as pl
from jax.experimental.pallas import tpu as pltpu
from jax.sharding import PartitionSpec as P

HEADS = 16
NARROW_HEAD_DIM = 64
GROUPS = 4
LANES = 128
RIM = 16

NORM_EPS = 1e-06
CLAMP_LIMIT = 7.0
SIGMOID_SCALE = 1.702

BF16, F32 = jnp.bfloat16, jnp.float32


def sigmoid(v):
    return 0.5 * jnp.tanh(0.5 * v) + 0.5


def dot(a, b):
    return jnp.dot(a, b, preferred_element_type=F32)


def layer_kernel(
    side,
    experts,
    capacity,
    resid_hbm,
    narrow_hbm,
    wide_hbm,
    key_hbm,
    query_hbm,
    narrow_gate_hbm,
    wide_gate_hbm,
    step_hbm,
    decay_ref,
    position_hbm,
    direct_ref,
    narrow_taps_hbm,
    wide_taps_hbm,
    key_taps_hbm,
    query_taps_hbm,
    narrow_gain_hbm,
    wide_gain_hbm,
    narrow_rows_hbm,
    wide_rows_hbm,
    gain_hbm,
    routes_hbm,
    route_weights_hbm,
    gate_hbm,
    up_hbm,
    down_hbm,
    out_ref,
    wide_in,
    narrow_in,
    wide_gate_v,
    narrow_gate_v,
    step_v,
    position_v,
    narrow_taps,
    wide_taps,
    key_taps,
    query_taps,
    narrow_gain,
    wide_gain,
    head_rows_v,
    gain_v,
    routes_v,
    route_weights_v,
    resid_v,
    gate_v,
    up_v,
    down_v,
    step_rows,
    decay_rows,
    mix,
    mix_low,
    key_mix,
    query_mix,
    scores,
    base,
    gate_act,
    states,
    state_out,
    pair_in,
    chain_in,
    chain_out,
    enter,
    factor_out,
    factor_in,
    head_out,
    head_part,
    head_in1,
    head_mid,
    head_in2,
    hidden,
    hidden_low,
    chooser,
    weight_high,
    weight_low,
    dispatch_out,
    tokens,
    partial,
    sum_in1,
    sum_mid,
    sum_in2,
    done_out,
    done_in,
    load_sem,
    rim_send,
    rim_recv,
    pair_send,
    pair_recv,
    chain_send,
    chain_recv,
    relay_send,
    relay_recv,
    head_sems,
    head_sems2,
    dispatch_send,
    dispatch_recv,
    own_send,
    own_recv,
    pass_send,
    pass_recv,
    sum_sems,
    sum_sems2,
    done_send,
    done_recv,
):
    me_s = lax.axis_index("sp")
    me_t = lax.axis_index("tp")
    col = me_t % side
    row = me_t // side
    core = me_s % 2
    plane = me_s // 2
    planes = experts // 2
    length, width = resid_v.shape
    shards = side * side
    groups = tokens.shape[1]
    sources = experts // groups
    state = key_hbm.shape[1] // GROUPS
    head_count = decay_ref.shape[1]
    wide_width = wide_hbm.shape[1]
    narrow_width = narrow_hbm.shape[1]
    peers = range(1, side)
    wide_columns = wide_width // LANES
    columns = []
    for i in range(wide_columns):
        columns.append((i * LANES, LANES, (head_count + i,)))
    for i in range(-(-narrow_width // LANES)):
        size = min(LANES, narrow_width - i * LANES)
        first = i * (LANES // NARROW_HEAD_DIM)
        columns.append(
            (i * LANES, size, tuple(first + k for k in range(size // NARROW_HEAD_DIM)))
        )
    column_count = len(columns)

    def at(c, r):
        return r * side + c

    def remote(src, dst, send, recv, where):
        return pltpu.make_async_remote_copy(
            src_ref=src,
            dst_ref=dst,
            send_sem=send,
            recv_sem=recv,
            device_id=where,
            device_id_type=pl.DeviceIdType.MESH,
        )

    group_column = pl.multiple_of(me_t * head_count // (HEADS // GROUPS) * state, LANES)
    own_columns = pl.ds(pl.multiple_of(me_t * width, LANES), width)
    group_slice = pl.ds(group_column, state)
    body = pl.ds(RIM, length)
    moves = (
        (wide_hbm, wide_in.at[body, pl.ds(0, wide_width)]),
        (key_hbm.at[:, group_slice], wide_in.at[body, pl.ds(wide_width, state)]),
        (query_hbm.at[:, group_slice], wide_in.at[body, pl.ds(wide_width + state, state)]),
        (narrow_hbm, narrow_in.at[body]),
        (wide_taps_hbm, wide_taps),
        (key_taps_hbm.at[:, group_slice], key_taps),
        (query_taps_hbm.at[:, group_slice], query_taps),
        (narrow_taps_hbm, narrow_taps),
        (step_hbm, step_v),
        (position_hbm, position_v),
        (wide_gate_hbm, wide_gate_v),
        (narrow_gate_hbm, narrow_gate_v),
        (narrow_gain_hbm, narrow_gain),
        (wide_gain_hbm, wide_gain),
        (routes_hbm, routes_v),
        (route_weights_hbm, route_weights_v),
        (wide_rows_hbm, head_rows_v.at[pl.ds(0, wide_width)]),
        (narrow_rows_hbm, head_rows_v.at[pl.ds(wide_width, narrow_width)]),
        (resid_hbm.at[:, own_columns], resid_v),
        (gain_hbm, gain_v),
        (gate_hbm.at[0], gate_v),
        (up_hbm.at[0], up_v),
        (down_hbm.at[0], down_v),
    )
    loads = [pltpu.make_async_copy(s, d, load_sem.at[i]) for i, (s, d) in enumerate(moves)]
    for load in loads:
        load.start()

    barrier = pltpu.get_barrier_semaphore()

    def greet(s, t):
        pl.semaphore_signal(
            barrier, inc=1, device_id=(s, t), device_id_type=pl.DeviceIdType.MESH
        )

    def greet_sp(d, c):
        greet((me_s + d) % experts, me_t)
        return c

    lax.fori_loop(1, experts, greet_sp, 0)
    for k in peers:
        greet(me_s, at((col + k) % side, row))
        greet(me_s, at(col, (row + k) % side))
    pl.semaphore_wait(barrier, experts - 1 + 2 * (side - 1))

    for load in loads[:4]:
        load.wait()

    tail = pl.ds(length, RIM)
    head = pl.ds(0, RIM)

    def rim_copies():
        where = (me_s + 1, me_t)
        return (
            remote(wide_in.at[tail], wide_in.at[head], rim_send.at[0], rim_recv.at[0], where),
            remote(narrow_in.at[tail], narrow_in.at[head], rim_send.at[1], rim_recv.at[1], where),
        )

    @pl.when(me_s < experts - 1)
    def _():
        for copy in rim_copies():
            copy.start()

    @pl.when(me_s == 0)
    def _():
        wide_in[:RIM, :] = jnp.zeros((RIM, wide_in.shape[1]), BF16)
        narrow_in[:RIM, :] = jnp.zeros((RIM, narrow_in.shape[1]), BF16)

    for load in loads[4:10]:
        load.wait()

    def padded(v):
        if v.shape[1] == LANES:
            return v
        return jnp.concatenate([v, jnp.zeros((v.shape[0], LANES - v.shape[1]), v.dtype)], axis=1)

    def conv(source, offset, size, taps, tap_offset, first, count):
        rows = padded(source[first : first + count + RIM, offset : offset + size]).astype(F32)
        weights = padded(taps[:, tap_offset : tap_offset + size])
        total = weights[-1:] * rows
        last = taps.shape[0] - 1
        for k in range(1, last + 1):
            total = total + weights[last - k : last - k + 1] * pltpu.roll(rows, k, 0)
        total = total[RIM:]
        return total * sigmoid(total)

    def convolve(first, count):
        keep = slice(first, first + count)
        key_mix[keep, :] = conv(wide_in, wide_width, state, key_taps, 0, first, count)
        query_mix[keep, :] = conv(
            wide_in, wide_width + state, state, query_taps, 0, first, count
        ).astype(BF16)
        for j, (offset, size, _) in enumerate(columns):
            wide = j < wide_columns
            value = conv(
                wide_in if wide else narrow_in,
                offset,
                size,
                wide_taps if wide else narrow_taps,
                offset,
                first,
                count,
            )
            mix[j, keep, :] = value
            mix_low[j, keep, :] = value.astype(BF16)

    convolve(RIM, length - RIM)

    lane = lax.broadcasted_iota(jnp.int32, (1, LANES), 1)

    def spread(parts):
        if len(parts) == 1:
            return parts[0]
        return jnp.where(lane < NARROW_HEAD_DIM, parts[0], parts[1])

    step_rows[...] = jnp.ones(step_rows.shape, F32)
    decay_rows[...] = jnp.zeros(decay_rows.shape, F32)
    head_index = lax.broadcasted_iota(jnp.int32, (head_count, length), 0)
    for g in range(2):
        raw = step_v[g].astype(F32)
        soft = jnp.maximum(raw, 0.0) + jnp.log(1.0 + jnp.exp(-jnp.abs(raw)))
        rate = jnp.zeros((head_count, length), F32)
        for h in range(head_count):
            rate = jnp.where(head_index == h, decay_ref[g, h], rate)
        keep = slice(g * head_count, (g + 1) * head_count)
        step_rows[keep, :] = soft
        decay_rows[keep, :] = position_v[g] - jnp.exp(rate) * soft
    line = lax.broadcasted_iota(jnp.int32, (length, length), 0)
    across = lax.broadcasted_iota(jnp.int32, (length, length), 1)
    upto = jnp.where(line <= across, 1.0, 0.0).astype(BF16)
    decays = decay_rows[...]
    high = decays.astype(BF16)
    middle = (decays - high.astype(F32)).astype(BF16)
    low = (decays - high.astype(F32) - middle.astype(F32)).astype(BF16)
    running = dot(high, upto) + (dot(middle, upto) + dot(low, upto))
    rows_kept = running.shape[0]
    total_decay = running[:, length - 1 : length]
    log_step = jnp.log(step_rows[...])
    offset_rows = running - log_step
    tail_rows = jnp.exp(total_decay - offset_rows)
    factors = jnp.exp(total_decay)
    running_columns = jnp.transpose(
        jnp.concatenate([running, jnp.zeros((LANES - rows_kept, length), F32)], axis=0)
    )
    factor_rows = []
    for _, _, heads in columns:
        parts = [jnp.broadcast_to(factors[h : h + 1, :], (1, LANES)) for h in heads]
        factor_rows.append(spread(parts))
    for j, value in enumerate(factor_rows):
        factor_out[j : j + 1, :] = value

    @pl.when(me_s > 0)
    def _():
        for copy in rim_copies():
            copy.wait_recv()

    convolve(0, RIM)

    key_turned = jnp.transpose(key_mix[...])
    for j, (_, _, heads) in enumerate(columns):
        parts = [
            dot((key_turned * tail_rows[h : h + 1, :]).astype(BF16), mix_low[j]) for h in heads
        ]
        states[j] = spread(parts)

    partner = me_s + 1 - 2 * core

    def pair_copy(j):
        if j == column_count:
            return remote(
                factor_out, factor_in, pair_send.at[j], pair_recv.at[j], (partner, me_t)
            )
        return remote(
            state_out.at[j], pair_in.at[j], pair_send.at[j], pair_recv.at[j], (partner, me_t)
        )

    @pl.when(core == 0)
    def _():
        pair_copy(column_count).start()
        for j in range(column_count):
            state_out[j] = states[j].astype(BF16)
            pair_copy(j).start()

    scores[...] = dot(query_mix[...], key_turned.astype(BF16))
    half = length // 2
    below = lax.broadcasted_iota(jnp.int32, (half, half), 0)
    beside = lax.broadcasted_iota(jnp.int32, (half, half), 1)
    causal = below >= beside

    def direct_row(heads):
        parts = []
        for h in heads:
            value = direct_ref[h // head_count, h % head_count]
            parts.append(jnp.full((1, LANES), value, F32))
        return spread(parts)

    def inside(j):
        heads = columns[j][2]
        parts = []
        for h in heads:
            up_to = running_columns[:, h : h + 1]
            since = offset_rows[h : h + 1, :]
            top = jnp.where(causal, up_to[:half] - since[:, :half], -1e30)
            left = up_to[half:] - since[:, :half]
            right = jnp.where(causal, up_to[half:] - since[:, half:], -1e30)
            upper = dot(
                (scores[:half, :half] * jnp.exp(top)).astype(BF16), mix_low[j, :half, :]
            )
            lower = dot(
                (scores[half:, :half] * jnp.exp(left)).astype(BF16), mix_low[j, :half, :]
            ) + dot((scores[half:, half:] * jnp.exp(right)).astype(BF16), mix_low[j, half:, :])
            parts.append((upper, lower))
        direct = direct_row(heads)
        base[j, :half, :] = spread([p[0] for p in parts]) + direct * mix[j, :half, :]
        base[j, half:, :] = spread([p[1] for p in parts]) + direct * mix[j, half:, :]

    early = min(2, column_count)
    for j in range(early):
        inside(j)

    def chain_copy(j):
        return remote(
            chain_out.at[j], chain_in.at[j], chain_send.at[j], chain_recv.at[j], (me_s + 2, me_t)
        )

    def relay_copy(j):
        return remote(
            chain_in.at[j], chain_in.at[j], relay_send.at[j], relay_recv.at[j], (me_s - 1, me_t)
        )

    @pl.when(core == 1)
    def _():
        pair_copy(column_count).wait_recv()
        for j in range(column_count):
            pair_copy(j).wait_recv()
            states[j] += factor_out[j : j + 1, :] * pair_in[j].astype(F32)

    @pl.when(jnp.logical_and(core == 1, plane == 0))
    def _():
        for j in range(column_count):
            if planes > 1:
                chain_out[j] = states[j].astype(BF16)
                chain_copy(j).start()
            enter[j] = pair_in[j]

    @pl.when(jnp.logical_and(core == 0, plane == 0))
    def _():
        enter[...] = jnp.zeros(enter.shape, BF16)

    for j in range(early, column_count):
        inside(j)

    for load in loads[10:16]:
        load.wait()

    for j, (offset, size, _) in enumerate(columns):
        source = wide_gate_v if j < wide_columns else narrow_gate_v
        value = padded(source[:, offset : offset + size]).astype(F32)
        gate_act[j] = value * sigmoid(value)

    @pl.when(jnp.logical_and(core == 1, plane > 0))
    def _():
        for j in range(column_count):
            chain_copy(j).wait_recv()
            relay_copy(j).start()
            carried = chain_in[j].astype(F32)
            moved = factor_in[j : j + 1, :] * carried

            @pl.when(plane < planes - 1)
            def _():
                chain_out[j] = (states[j] + factor_out[j : j + 1, :] * moved).astype(BF16)
                chain_copy(j).start()

            enter[j] = (pair_in[j].astype(F32) + moved).astype(BF16)

    order = lax.broadcasted_iota(jnp.int32, (experts, length), 0)
    order = jnp.where(order == 0, 0, jnp.where(order == experts - 1, 1, order + 1))
    place = plane + lax.shift_right_logical(order, 1)
    place = jnp.where(place >= planes, place - planes, place)
    flip = core + (order & 1)
    flip = jnp.where(flip >= 2, flip - 2, flip)
    named = place * 2 + flip
    member = jnp.zeros((experts, length), F32)
    weight_rows = jnp.zeros((experts, length), F32)
    for k in range(routes_v.shape[0]):
        hit = routes_v[k : k + 1, :] == named
        member = jnp.where(hit, 1.0, member)
        weight_rows = jnp.where(hit, route_weights_v[k : k + 1, :], weight_rows)
    before = jnp.where(line < across, 1.0, 0.0).astype(BF16)
    ranks = dot(member.astype(BF16), before)
    ranks = jnp.where(member > 0.5, ranks, -1.0)
    slots = lax.broadcasted_iota(jnp.int32, (capacity, length), 0).astype(F32)
    slot_lanes = lax.broadcasted_iota(jnp.int32, (length, capacity), 1).astype(F32)
    filler = [jnp.zeros((LANES - experts, length), F32)] if experts < LANES else []
    rank_columns = jnp.transpose(jnp.concatenate([ranks] + filler, axis=0))
    weight_columns = jnp.transpose(jnp.concatenate([weight_rows] + filler, axis=0))
    for d in range(experts):
        chooser[d] = jnp.where(slots == ranks[d : d + 1, :], 1.0, 0.0).astype(BF16)
        weights = jnp.where(
            slot_lanes == rank_columns[:, d : d + 1], weight_columns[:, d : d + 1], 0.0
        )
        rounded = weights.astype(BF16)
        weight_high[d] = rounded
        weight_low[d] = (weights - rounded.astype(F32)).astype(BF16)

    @pl.when(jnp.logical_and(core == 0, plane > 0))
    def _():
        for j in range(column_count):
            relay_copy(j).wait_recv()
            enter[j] = chain_in[j]

    for j, (offset, size, heads) in enumerate(columns):
        wide = j < wide_columns
        grown = spread([jnp.exp(running_columns[:, h : h + 1]) for h in heads])
        value = (base[j] + grown * dot(query_mix[...], enter[j])) * gate_act[j]
        square = value * value
        if len(heads) == 1:
            total = jnp.sum(square, axis=1, keepdims=True)
        else:
            first = jnp.sum(jnp.where(lane < NARROW_HEAD_DIM, square, 0.0), axis=1, keepdims=True)
            rest = jnp.sum(jnp.where(lane < NARROW_HEAD_DIM, 0.0, square), axis=1, keepdims=True)
            total = spread([first, rest])
        value = value * lax.rsqrt(total / (size // len(heads)) + NORM_EPS)
        gains = padded((wide_gain if wide else narrow_gain)[:, offset : offset + size])
        value = (value * gains).astype(BF16)
        start = offset if wide else wide_width + offset
        head_out[:, start : start + size] = value[:, :size]

    for load in loads[16:20]:
        load.wait()

    def first_copy(bundle, dim, k, other, d):
        part, in1, _, _, sems, _ = bundle
        rows = in1.shape[4]
        if dim == 0:
            block = at((col + k) % side, (row + other) % side)
            peer = at((col + k) % side, row)
        else:
            block = at((col + other) % side, (row + k) % side)
            peer = at(col, (row + k) % side)
        return remote(
            part.at[d, block, pl.ds(dim * rows, rows)],
            in1.at[dim, k - 1, other, d],
            sems.at[0, dim, k - 1, other, d],
            sems.at[1, dim, k - 1, other, d],
            (me_s, peer),
        )

    def second_copy(bundle, dim, k, d):
        _, _, mid, in2, _, sems = bundle
        peer = at(col, (row + k) % side) if dim == 0 else at((col + k) % side, row)
        return remote(
            mid.at[dim, k - 1, d],
            in2.at[dim, k - 1, d],
            sems.at[0, dim, k - 1, d],
            sems.at[1, dim, k - 1, d],
            (me_s, peer),
        )

    def scatter(bundle, d, produce):
        part = bundle[0]
        shifts = [(a, b) for a in range(side) for b in range(side)]
        shifts.sort(key=lambda s: -((s[0] > 0) + (s[1] > 0)))
        for a, b in shifts:
            block = at((col + a) % side, (row + b) % side)
            part[d, block] = produce(block).astype(BF16)
            if a:
                first_copy(bundle, 0, a, b, d).start()
            if b:
                first_copy(bundle, 1, b, a, d).start()

    def forward(bundle, d):
        part, in1, mid, _, _, _ = bundle
        rows = in1.shape[4]
        for k in peers:
            for dim in range(2):
                block = at(col, (row + k) % side) if dim == 0 else at((col + k) % side, row)
                total = part[d, block, dim * rows : (dim + 1) * rows].astype(F32)
                for j in peers:
                    first_copy(bundle, dim, j, k, d).wait_recv()
                    total = total + in1[dim, j - 1, k, d].astype(F32)
                mid[dim, k - 1, d] = total.astype(BF16)
                second_copy(bundle, dim, k, d).start()

    def gathered(bundle, dim, d):
        part, in1, _, in2, _, _ = bundle
        rows = in1.shape[4]
        total = part[d, me_t, dim * rows : (dim + 1) * rows].astype(F32)
        for j in peers:
            first_copy(bundle, dim, j, 0, d).wait_recv()
            total = total + in1[dim, j - 1, 0, d].astype(F32)
        for k in peers:
            second_copy(bundle, dim, k, d).wait_recv()
            total = total + in2[dim, k - 1, d].astype(F32)
        return total

    def sent(bundle, d):
        for k in peers:
            for dim in range(2):
                for other in range(side):
                    first_copy(bundle, dim, k, other, d).wait_send()
                second_copy(bundle, dim, k, d).wait_send()

    def project(block):
        lanes = pl.ds(pl.multiple_of(block * width, LANES), width)
        return dot(head_out[...], head_rows_v[:, lanes])

    heads_bundle = (head_part, head_in1, head_mid, head_in2, head_sems, head_sems2)
    sums_bundle = (partial, sum_in1, sum_mid, sum_in2, sum_sems, sum_sems2)
    scatter(heads_bundle, 0, project)
    forward(heads_bundle, 0)
    for dim in range(2):
        keep = slice(dim * half, (dim + 1) * half)
        value = gathered(heads_bundle, dim, 0) + resid_v[keep, :].astype(F32)
        hidden[keep, :] = value
        hidden_low[keep, :] = value.astype(BF16)

    def pick(d):
        return dot(chooser[d], hidden_low[...]).astype(BF16)

    def target(d):
        index = d % (experts - 1) + 1
        return ((plane + index // 2) % planes) * 2 + (core + index % 2) % 2

    def source(d):
        index = d % (experts - 1) + 1
        return ((plane + planes - index // 2) % planes) * 2 + (core + index % 2) % 2

    def slot(d):
        return pl.ds((d % sources) * capacity, capacity)

    def dispatch_copy(d):
        return remote(
            dispatch_out.at[d],
            tokens.at[me_t, d // sources, slot(d)],
            dispatch_send.at[d],
            dispatch_recv.at[d],
            (target(d), me_t),
        )

    def done_copy(d):
        return remote(
            done_out.at[d // sources, slot(d)],
            done_in.at[d],
            done_send.at[d],
            done_recv.at[d],
            (source(d), me_t),
        )

    def send_dispatch(d, c):
        dispatch_out[d] = pick(d)
        dispatch_copy(d).start()
        return c

    tokens[me_t, 0, :capacity] = pick(0)

    def own_copy(dim, k, d):
        part = tokens.at[me_t, d]
        peer = at((col + k) % side, row) if dim == 0 else at(col, (row + k) % side)
        return remote(
            part, part, own_send.at[dim, k - 1, d], own_recv.at[dim, k - 1, d], (me_s, peer)
        )

    rows = tokens.shape[2] // 2

    def pass_copy(dim, j, k, d):
        if dim == 0:
            block = at((col + side - j) % side, row)
            peer = at(col, (row + k) % side)
        else:
            block = at(col, (row + side - j) % side)
            peer = at((col + k) % side, row)
        part = tokens.at[block, d, pl.ds(dim * rows, rows)]
        return remote(
            part,
            part,
            pass_send.at[dim, j - 1, k - 1, d],
            pass_recv.at[dim, j - 1, k - 1, d],
            (me_s, peer),
        )

    def expert(d):
        pieces = [tokens[j, d].astype(F32) for j in range(shards)]
        square = jnp.zeros((2 * rows, 1), F32)
        for piece in pieces:
            square = square + jnp.sum(piece * piece, axis=1, keepdims=True)
        scale = lax.rsqrt(square / (shards * width) + NORM_EPS)
        normed = jnp.concatenate(
            [
                (piece * scale * gain_v[:, j * width : (j + 1) * width]).astype(BF16)
                for j, piece in enumerate(pieces)
            ],
            axis=1,
        )
        gate = dot(normed, gate_v[...])
        up = dot(normed, up_v[...])
        clamped = jnp.minimum(gate, CLAMP_LIMIT)
        act = (
            (jnp.clip(up, -CLAMP_LIMIT, CLAMP_LIMIT) + 1.0)
            * clamped
            * sigmoid(SIGMOID_SCALE * clamped)
        ).astype(BF16)

        def down(block):
            lanes = pl.ds(pl.multiple_of(block * width, LANES), width)
            return dot(act, down_v[:, lanes])

        scatter(sums_bundle, d, down)

    def combine(d, block):
        hidden[...] += dot(weight_high[d], block) + dot(weight_low[d], block)

    def within(value):
        return jnp.logical_and(value >= 0, value < groups)

    def take_done(d, c):
        @pl.when(d == 0)
        def _():
            combine(0, done_out[0, :capacity])

        @pl.when(d > 0)
        def _():
            done_copy(d).wait_recv()
            combine(d, done_in[d])

        return c

    lag = 6

    def step(i, c):
        @pl.when(within(i - 1))
        def _():
            for k in peers:
                for dim in range(2):
                    own_copy(dim, k, i - 1).wait_recv()
            for dim in range(2):
                for j in peers:
                    for k in peers:
                        pass_copy(dim, j, k, i - 1).start()

        @pl.when(i < groups)
        def _():
            def arrive(d, c):
                @pl.when(d > 0)
                def _():
                    dispatch_copy(d).wait_recv()

                return c

            lax.fori_loop(i * sources, (i + 1) * sources, arrive, 0)
            for k in peers:
                for dim in range(2):
                    own_copy(dim, k, i).start()

        @pl.when(i == 0)
        def _():
            if sources == 1:
                lax.fori_loop(1, experts, send_dispatch, 0)
            for load in loads[20:]:
                load.wait()

        @pl.when(within(i - 3))
        def _():
            forward(sums_bundle, i - 3)

        @pl.when(within(i - 2))
        def _():
            for dim in range(2):
                for j in peers:
                    for k in peers:
                        pass_copy(dim, j, k, i - 2).wait_recv()
            expert(i - 2)

        @pl.when(within(i - 4))
        def _():
            for dim in range(2):
                done_out[i - 4, dim * rows : (dim + 1) * rows] = gathered(
                    sums_bundle, dim, i - 4
                ).astype(BF16)

            def leave(d, c):
                @pl.when(d > 0)
                def _():
                    done_copy(d).start()

                return c

            lax.fori_loop((i - 4) * sources, (i - 3) * sources, leave, 0)

        @pl.when(within(i - lag))
        def _():
            lax.fori_loop((i - lag) * sources, (i - lag + 1) * sources, take_done, 0)

        return c

    steps = groups + 4
    if sources > 1:
        lax.fori_loop(1, experts, send_dispatch, 0)
    lax.fori_loop(0, steps, step, 0)
    lax.fori_loop((steps - lag) * sources, experts, take_done, 0)
    out_ref[...] = hidden[...].astype(BF16)

    @pl.when(me_s < experts - 1)
    def _():
        for copy in rim_copies():
            copy.wait_send()

    @pl.when(core == 0)
    def _():
        for j in range(column_count + 1):
            pair_copy(j).wait_send()

    @pl.when(jnp.logical_and(core == 1, plane < planes - 1))
    def _():
        for j in range(column_count):
            chain_copy(j).wait_send()

    @pl.when(jnp.logical_and(core == 1, plane > 0))
    def _():
        for j in range(column_count):
            relay_copy(j).wait_send()

    sent(heads_bundle, 0)

    def finish_sp(d, c):
        dispatch_copy(d).wait_send()
        done_copy(d).wait_send()
        return c

    lax.fori_loop(1, experts, finish_sp, 0)

    def finish_group(d, c):
        for dim in range(2):
            for j in peers:
                own_copy(dim, j, d).wait_send()
                for k in peers:
                    pass_copy(dim, j, k, d).wait_send()
        sent(sums_bundle, d)
        return c

    lax.fori_loop(0, groups, finish_group, 0)


def layer_call(side, experts, arrays):
    resid, narrow, wide, key = arrays[:4]
    step, decay = arrays[7], arrays[8]
    gate, up, down = arrays[22:]
    routes = arrays[20]
    length = resid.shape[0]
    shards = side * side
    width = resid.shape[1] // shards
    capacity = 4 * length * routes.shape[0] // (3 * experts)
    sources = max(1, min(experts, 128 // capacity))
    groups = experts // sources
    rows = sources * capacity
    state = key.shape[1] // GROUPS
    wide_width, narrow_width = wide.shape[1], narrow.shape[1]
    column_count = wide_width // LANES + -(-narrow_width // LANES)
    head_rows = wide_width + narrow_width
    near = side - 1
    tap_count = arrays[11].shape[0]
    vmem = pltpu.VMEM
    dma = pltpu.SemaphoreType.DMA
    scratch = [
        vmem((RIM + length, wide_width + 2 * state), BF16),
        vmem((RIM + length, narrow_width), BF16),
        vmem((length, wide_width), BF16),
        vmem((length, narrow_width), BF16),
        vmem(step.shape, BF16),
        vmem(step.shape, F32),
        vmem((tap_count, narrow_width), F32),
        vmem((tap_count, wide_width), F32),
        vmem((tap_count, state), F32),
        vmem((tap_count, state), F32),
        vmem((1, narrow_width), F32),
        vmem((1, wide_width), F32),
        vmem((head_rows, resid.shape[1]), BF16),
        vmem((1, resid.shape[1]), F32),
        vmem(routes.shape, jnp.int32),
        vmem(routes.shape, F32),
        vmem((length, width), BF16),
        vmem(gate.shape[1:], BF16),
        vmem(up.shape[1:], BF16),
        vmem(down.shape[1:], BF16),
        vmem((8, length), F32),
        vmem((8, length), F32),
        vmem((column_count, length, LANES), F32),
        vmem((column_count, length, LANES), BF16),
        vmem((length, state), F32),
        vmem((length, state), BF16),
        vmem((length, length), F32),
        vmem((column_count, length, LANES), F32),
        vmem((column_count, length, LANES), F32),
        vmem((column_count, state, LANES), F32),
        vmem((column_count, state, LANES), BF16),
        vmem((column_count, state, LANES), BF16),
        vmem((column_count, state, LANES), BF16),
        vmem((column_count, state, LANES), BF16),
        vmem((column_count, state, LANES), BF16),
        vmem((8, LANES), F32),
        vmem((8, LANES), F32),
        vmem((length, head_rows), BF16),
        vmem((1, shards, length, width), BF16),
        vmem((2, near, side, 1, length // 2, width), BF16),
        vmem((2, near, 1, length // 2, width), BF16),
        vmem((2, near, 1, length // 2, width), BF16),
        vmem((length, width), F32),
        vmem((length, width), BF16),
        vmem((experts, capacity, length), BF16),
        vmem((experts, length, capacity), BF16),
        vmem((experts, length, capacity), BF16),
        vmem((experts, capacity, width), BF16),
        vmem((shards, groups, rows, width), BF16),
        vmem((groups, shards, rows, width), BF16),
        vmem((2, near, side, groups, rows // 2, width), BF16),
        vmem((2, near, groups, rows // 2, width), BF16),
        vmem((2, near, groups, rows // 2, width), BF16),
        vmem((groups, rows, width), BF16),
        vmem((experts, capacity, width), BF16),
        dma((23,)),
        dma((2,)),
        dma((2,)),
        dma((column_count + 1,)),
        dma((column_count + 1,)),
        dma((column_count,)),
        dma((column_count,)),
        dma((column_count,)),
        dma((column_count,)),
        dma((2, 2, near, side, 1)),
        dma((2, 2, near, 1)),
        dma((experts,)),
        dma((experts,)),
        dma((2, near, groups)),
        dma((2, near, groups)),
        dma((2, near, near, groups)),
        dma((2, near, near, groups)),
        dma((2, 2, near, side, groups)),
        dma((2, 2, near, groups)),
        dma((experts,)),
        dma((experts,)),
    ]
    hbm = pl.BlockSpec(memory_space=pl.ANY)
    smem = pl.BlockSpec(memory_space=pltpu.SMEM)
    specs = [hbm] * len(arrays)
    specs[8] = smem
    specs[10] = smem
    return pl.pallas_call(
        functools.partial(layer_kernel, side, experts, capacity),
        out_shape=jax.ShapeDtypeStruct((length, width), BF16),
        in_specs=specs,
        out_specs=pl.BlockSpec(memory_space=pltpu.VMEM),
        scratch_shapes=scratch,
        compiler_params=pltpu.CompilerParams(
            collective_id=0, has_side_effects=True, vmem_limit_bytes=60 * 1024 * 1024
        ),
    )(*arrays)


def local(*arrays):
    arrays = list(arrays)
    shards = lax.axis_size("tp")
    side = int(round(shards**0.5))
    assert side * side == shards
    for i in (7, 9):
        arrays[i] = jnp.transpose(arrays[i], (1, 2, 0))
    for i in (15, 16, 19):
        arrays[i] = arrays[i][None, :]
    for i in (20, 21):
        arrays[i] = jnp.transpose(arrays[i])
    return layer_call(side, lax.axis_size("sp"), arrays)


def solution(mesh):
    return jax.shard_map(
        local,
        mesh=mesh,
        in_specs=(
            P("sp", None),
            P("sp", "tp"),
            P("sp", "tp"),
            P("sp", None),
            P("sp", None),
            P("sp", "tp"),
            P("sp", "tp"),
            P("sp", None, "tp"),
            P(None, "tp"),
            P("sp", None, "tp"),
            P(None, "tp"),
            P(None, "tp"),
            P(None, "tp"),
            P(),
            P(),
            P("tp"),
            P("tp"),
            P("tp", None),
            P("tp", None),
            P(),
            P("sp", None),
            P("sp", None),
            P("sp", None, "tp"),
            P("sp", None, "tp"),
            P("sp", "tp", None),
        ),
        out_specs=P("sp", "tp"),
        check_vma=False,
    )
```

```python
import functools

import jax
import jax.numpy as jnp
from jax import lax
from jax.experimental import pallas as pl
from jax.experimental.pallas import tpu as pltpu
from jax.sharding import PartitionSpec as P

HEADS = 16
NARROW_HEAD_DIM = 64
GROUPS = 4
LANES = 128
RIM = 16
FAR_GROUPS = 2

NORM_EPS = 1e-06
CLAMP_LIMIT = 7.0
SIGMOID_SCALE = 1.702

BF16, F32 = jnp.bfloat16, jnp.float32


def sigmoid(v):
    return 0.5 * jnp.tanh(0.5 * v) + 0.5


def dot(a, b):
    return jnp.dot(a, b, preferred_element_type=F32)


def layer_kernel(
    side,
    experts,
    capacity,
    resid_hbm,
    narrow_hbm,
    wide_hbm,
    key_hbm,
    query_hbm,
    narrow_gate_hbm,
    wide_gate_hbm,
    step_hbm,
    decay_ref,
    position_hbm,
    direct_ref,
    narrow_taps_hbm,
    wide_taps_hbm,
    key_taps_hbm,
    query_taps_hbm,
    narrow_gain_hbm,
    wide_gain_hbm,
    narrow_rows_hbm,
    wide_rows_hbm,
    gain_hbm,
    routes_hbm,
    route_weights_hbm,
    gate_hbm,
    up_hbm,
    down_hbm,
    out_ref,
    rim_wide,
    rim_narrow,
    wide_in,
    narrow_in,
    wide_gate_v,
    narrow_gate_v,
    step_v,
    position_v,
    narrow_taps,
    wide_taps,
    key_taps,
    query_taps,
    narrow_gain,
    wide_gain,
    head_rows_v,
    gain_v,
    routes_v,
    route_weights_v,
    resid_v,
    gate_v,
    up_v,
    down_v,
    step_rows,
    decay_rows,
    mix,
    mix_low,
    key_mix,
    query_mix,
    scores,
    base,
    gate_act,
    states,
    state_out,
    pair_in,
    chain_in,
    chain_out,
    enter,
    factor_out,
    factor_in,
    head_out,
    head_part,
    head_in1,
    head_mid,
    head_in2,
    hidden,
    chooser,
    weight_high,
    weight_low,
    dispatch_out,
    tokens,
    partial,
    sum_in1,
    sum_mid,
    sum_in2,
    done_out,
    done_in,
    full,
    partner_out,
    far_out,
    out_v,
    load_sem,
    rim_send,
    rim_recv,
    pair_send,
    pair_recv,
    chain_send,
    chain_recv,
    relay_send,
    relay_recv,
    head_sems,
    early_sems,
    dispatch_send,
    dispatch_recv,
    far_send,
    far_recv,
    token_sems,
    sum_sems,
    done_send,
    done_recv,
):
    me_s = lax.axis_index("sp")
    me_t = lax.axis_index("tp")
    col = me_t % side
    row = me_t // side
    core = me_s % 2
    plane = me_s // 2
    planes = experts // 2
    length, width = resid_v.shape
    shards = side * side
    groups = tokens.shape[1]
    sources = experts // groups
    state = key_hbm.shape[1] // GROUPS
    head_count = decay_ref.shape[1]
    wide_width = wide_hbm.shape[1]
    narrow_width = narrow_hbm.shape[1]
    peers = range(1, side)
    wide_columns = wide_width // LANES
    columns = []
    for i in range(wide_columns):
        columns.append((i * LANES, LANES, (head_count + i,)))
    for i in range(-(-narrow_width // LANES)):
        size = min(LANES, narrow_width - i * LANES)
        first = i * (LANES // NARROW_HEAD_DIM)
        columns.append(
            (i * LANES, size, tuple(first + k for k in range(size // NARROW_HEAD_DIM)))
        )
    column_count = len(columns)

    def at(c, r):
        return r * side + c

    def remote(src, dst, send, recv, where):
        return pltpu.make_async_remote_copy(
            src_ref=src,
            dst_ref=dst,
            send_sem=send,
            recv_sem=recv,
            device_id=where,
            device_id_type=pl.DeviceIdType.MESH,
        )

    group_column = pl.multiple_of(me_t * head_count // (HEADS // GROUPS) * state, LANES)
    own_columns = pl.ds(pl.multiple_of(me_t * width, LANES), width)
    group_slice = pl.ds(group_column, state)
    body = pl.ds(RIM, length)
    edge = pl.ds(length - RIM, RIM)
    wide_part = pl.ds(0, wide_width)
    key_part = pl.ds(wide_width, state)
    query_part = pl.ds(wide_width + state, state)
    moves = (
        (0, wide_hbm.at[edge], rim_wide.at[:, wide_part]),
        (0, key_hbm.at[edge, group_slice], rim_wide.at[:, key_part]),
        (0, query_hbm.at[edge, group_slice], rim_wide.at[:, query_part]),
        (1, narrow_hbm.at[edge], rim_narrow),
        (2, wide_hbm, wide_in.at[body, wide_part]),
        (2, key_hbm.at[:, group_slice], wide_in.at[body, key_part]),
        (2, query_hbm.at[:, group_slice], wide_in.at[body, query_part]),
        (3, narrow_hbm, narrow_in.at[body]),
        (4, wide_taps_hbm, wide_taps),
        (5, key_taps_hbm.at[:, group_slice], key_taps),
        (6, query_taps_hbm.at[:, group_slice], query_taps),
        (7, narrow_taps_hbm, narrow_taps),
        (8, step_hbm, step_v),
        (9, position_hbm, position_v),
        (10, wide_gate_hbm, wide_gate_v),
        (11, narrow_gate_hbm, narrow_gate_v),
        (12, narrow_gain_hbm, narrow_gain),
        (13, wide_gain_hbm, wide_gain),
        (14, routes_hbm, routes_v),
        (15, route_weights_hbm, route_weights_v),
        (16, wide_rows_hbm, head_rows_v.at[wide_part]),
        (16, narrow_rows_hbm, head_rows_v.at[pl.ds(wide_width, narrow_width)]),
        (17, resid_hbm.at[:, own_columns], resid_v),
        (18, gain_hbm, gain_v),
        (19, gate_hbm.at[0], gate_v),
        (20, up_hbm.at[0], up_v),
        (21, down_hbm.at[0], down_v),
    )
    whole = {0: rim_wide, 2: wide_in.at[body], 16: head_rows_v}

    def load(first, last):
        for i, source, target in moves:
            if first <= i < last:
                pltpu.make_async_copy(source, target, load_sem.at[i]).start()

    def spent(ref, sem):
        pltpu.make_async_copy(ref, ref, sem).wait()

    def loaded(first, last):
        for i in range(first, last):
            ref = whole.get(i, [m[2] for m in moves if m[0] == i][0])
            spent(ref, load_sem.at[i])

    barrier = pltpu.get_barrier_semaphore()

    def greet(s, t):
        pl.semaphore_signal(
            barrier, inc=1, device_id=(s, t), device_id_type=pl.DeviceIdType.MESH
        )

    def greet_sp(d, c):
        greet((me_s + d) % experts, me_t)
        return c

    load(0, 2)
    lax.fori_loop(1, experts, greet_sp, 0)
    for k in peers:
        greet(me_s, at((col + k) % side, row))
        greet(me_s, at(col, (row + k) % side))
    load(2, 16)
    loaded(0, 2)
    pl.semaphore_wait(barrier, experts - 1 + 2 * (side - 1))

    head = pl.ds(0, RIM)

    def rim_copies():
        where = (me_s + 1, me_t)
        return (
            remote(rim_wide, wide_in.at[head], rim_send.at[0], rim_recv.at[0], where),
            remote(rim_narrow, narrow_in.at[head], rim_send.at[1], rim_recv.at[1], where),
        )

    @pl.when(me_s < experts - 1)
    def _():
        for copy in rim_copies():
            copy.start()

    @pl.when(me_s == 0)
    def _():
        wide_in[:RIM, :] = jnp.zeros((RIM, wide_in.shape[1]), BF16)
        narrow_in[:RIM, :] = jnp.zeros((RIM, narrow_in.shape[1]), BF16)

    load(16, 22)
    loaded(2, 10)

    def padded(v):
        if v.shape[1] == LANES:
            return v
        return jnp.concatenate([v, jnp.zeros((v.shape[0], LANES - v.shape[1]), v.dtype)], axis=1)

    def conv(source, offset, size, taps, tap_offset, first, count):
        rows = padded(source[first : first + count + RIM, offset : offset + size]).astype(F32)
        weights = padded(taps[:, tap_offset : tap_offset + size])
        total = weights[-1:] * rows
        last = taps.shape[0] - 1
        for k in range(1, last + 1):
            total = total + weights[last - k : last - k + 1] * pltpu.roll(rows, k, 0)
        total = total[RIM:]
        return total * sigmoid(total)

    def convolve(first, count):
        keep = slice(first, first + count)
        key_mix[keep, :] = conv(wide_in, wide_width, state, key_taps, 0, first, count)
        query_mix[keep, :] = conv(
            wide_in, wide_width + state, state, query_taps, 0, first, count
        ).astype(BF16)
        for j, (offset, size, _) in enumerate(columns):
            wide = j < wide_columns
            value = conv(
                wide_in if wide else narrow_in,
                offset,
                size,
                wide_taps if wide else narrow_taps,
                offset,
                first,
                count,
            )
            mix[j, keep, :] = value
            mix_low[j, keep, :] = value.astype(BF16)

    convolve(RIM, length - RIM)

    lane = lax.broadcasted_iota(jnp.int32, (1, LANES), 1)

    def spread(parts):
        if len(parts) == 1:
            return parts[0]
        return jnp.where(lane < NARROW_HEAD_DIM, parts[0], parts[1])

    step_rows[...] = jnp.ones(step_rows.shape, F32)
    decay_rows[...] = jnp.zeros(decay_rows.shape, F32)
    head_index = lax.broadcasted_iota(jnp.int32, (head_count, length), 0)
    for g in range(2):
        raw = step_v[g].astype(F32)
        soft = jnp.maximum(raw, 0.0) + jnp.log(1.0 + jnp.exp(-jnp.abs(raw)))
        rate = jnp.zeros((head_count, length), F32)
        for h in range(head_count):
            rate = jnp.where(head_index == h, decay_ref[g, h], rate)
        keep = slice(g * head_count, (g + 1) * head_count)
        step_rows[keep, :] = soft
        decay_rows[keep, :] = position_v[g] - jnp.exp(rate) * soft
    line = lax.broadcasted_iota(jnp.int32, (length, length), 0)
    across = lax.broadcasted_iota(jnp.int32, (length, length), 1)
    upto = jnp.where(line <= across, 1.0, 0.0).astype(BF16)
    decays = decay_rows[...]
    high = decays.astype(BF16)
    middle = (decays - high.astype(F32)).astype(BF16)
    low = (decays - high.astype(F32) - middle.astype(F32)).astype(BF16)
    running = dot(high, upto) + (dot(middle, upto) + dot(low, upto))
    rows_kept = running.shape[0]
    total_decay = running[:, length - 1 : length]
    log_step = jnp.log(step_rows[...])
    offset_rows = running - log_step
    tail_rows = jnp.exp(total_decay - offset_rows)
    factors = jnp.exp(total_decay)
    running_columns = jnp.transpose(
        jnp.concatenate([running, jnp.zeros((LANES - rows_kept, length), F32)], axis=0)
    )
    factor_rows = []
    for _, _, heads in columns:
        parts = [jnp.broadcast_to(factors[h : h + 1, :], (1, LANES)) for h in heads]
        factor_rows.append(spread(parts))
    for j, value in enumerate(factor_rows):
        factor_out[j : j + 1, :] = value

    loaded(10, 16)

    for j, (offset, size, _) in enumerate(columns):
        source = wide_gate_v if j < wide_columns else narrow_gate_v
        value = padded(source[:, offset : offset + size]).astype(F32)
        gate_act[j] = value * sigmoid(value)

    order = lax.broadcasted_iota(jnp.int32, (experts, length), 0)
    mask = jnp.where(order < experts - 3, order + 3, order + 5 - experts)
    mask = jnp.where(order == 0, 1, jnp.where(order == experts - 1, 0, mask))
    named = mask ^ me_s
    member = jnp.zeros((experts, length), F32)
    weight_rows = jnp.zeros((experts, length), F32)
    for k in range(routes_v.shape[0]):
        hit = routes_v[k : k + 1, :] == named
        member = jnp.where(hit, 1.0, member)
        weight_rows = jnp.where(hit, route_weights_v[k : k + 1, :], weight_rows)
    before = jnp.where(line < across, 1.0, 0.0).astype(BF16)
    ranks = dot(member.astype(BF16), before)
    ranks = jnp.where(member > 0.5, ranks, -1.0)
    slots = lax.broadcasted_iota(jnp.int32, (capacity, length), 0).astype(F32)
    slot_lanes = lax.broadcasted_iota(jnp.int32, (length, capacity), 1).astype(F32)
    filler = [jnp.zeros((LANES - experts, length), F32)] if experts < LANES else []
    rank_columns = jnp.transpose(jnp.concatenate([ranks] + filler, axis=0))
    weight_columns = jnp.transpose(jnp.concatenate([weight_rows] + filler, axis=0))
    for d in range(experts):
        chooser[d] = jnp.where(slots == ranks[d : d + 1, :], 1.0, 0.0).astype(BF16)
        weights = jnp.where(
            slot_lanes == rank_columns[:, d : d + 1], weight_columns[:, d : d + 1], 0.0
        )
        rounded = weights.astype(BF16)
        weight_high[d] = rounded
        weight_low[d] = (weights - rounded.astype(F32)).astype(BF16)

    @pl.when(me_s > 0)
    def _():
        for copy in rim_copies():
            copy.wait_recv()

    convolve(0, RIM)

    key_turned = jnp.transpose(key_mix[...])
    for j, (_, _, heads) in enumerate(columns):
        parts = [
            dot((key_turned * tail_rows[h : h + 1, :]).astype(BF16), mix_low[j]) for h in heads
        ]
        states[j] = spread(parts)

    partner = me_s + 1 - 2 * core

    def pair_copy(j):
        if j == column_count:
            return remote(
                factor_out, factor_in, pair_send.at[1], pair_recv.at[1], (partner, me_t)
            )
        return remote(
            state_out.at[j], pair_in.at[j], pair_send.at[0], pair_recv.at[0], (partner, me_t)
        )

    @pl.when(core == 0)
    def _():
        pair_copy(column_count).start()
        for j in range(column_count):
            state_out[j] = states[j].astype(BF16)
            pair_copy(j).start()

    scores[...] = dot(query_mix[...], key_turned.astype(BF16))
    half = length // 2
    below = lax.broadcasted_iota(jnp.int32, (half, half), 0)
    beside = lax.broadcasted_iota(jnp.int32, (half, half), 1)
    causal = below >= beside

    def direct_row(heads):
        parts = []
        for h in heads:
            value = direct_ref[h // head_count, h % head_count]
            parts.append(jnp.full((1, LANES), value, F32))
        return spread(parts)

    def inside(j):
        heads = columns[j][2]
        parts = []
        for h in heads:
            up_to = running_columns[:, h : h + 1]
            since = offset_rows[h : h + 1, :]
            top = jnp.where(causal, up_to[:half] - since[:, :half], -1e30)
            left = up_to[half:] - since[:, :half]
            right = jnp.where(causal, up_to[half:] - since[:, half:], -1e30)
            upper = dot(
                (scores[:half, :half] * jnp.exp(top)).astype(BF16), mix_low[j, :half, :]
            )
            lower = dot(
                (scores[half:, :half] * jnp.exp(left)).astype(BF16), mix_low[j, :half, :]
            ) + dot((scores[half:, half:] * jnp.exp(right)).astype(BF16), mix_low[j, half:, :])
            parts.append((upper, lower))
        direct = direct_row(heads)
        base[j, :half, :] = spread([p[0] for p in parts]) + direct * mix[j, :half, :]
        base[j, half:, :] = spread([p[1] for p in parts]) + direct * mix[j, half:, :]

    early = min(2, column_count)
    for j in range(early):
        inside(j)

    def chain_copy(j):
        return remote(
            chain_out.at[j], chain_in.at[j], chain_send.at[0], chain_recv.at[j], (me_s + 2, me_t)
        )

    def relay_copy(j):
        return remote(
            chain_in.at[j], chain_in.at[j], relay_send.at[0], relay_recv.at[j], (me_s - 1, me_t)
        )

    @pl.when(core == 1)
    def _():
        pair_copy(column_count).wait_recv()
        spent(pair_in, pair_recv.at[0])
        for j in range(column_count):
            states[j] += factor_out[j : j + 1, :] * pair_in[j].astype(F32)

    @pl.when(jnp.logical_and(core == 1, plane == 0))
    def _():
        for j in range(column_count):
            if planes > 1:
                chain_out[j] = states[j].astype(BF16)
                chain_copy(j).start()
            enter[j] = pair_in[j]

    @pl.when(jnp.logical_and(core == 0, plane == 0))
    def _():
        enter[...] = jnp.zeros(enter.shape, BF16)

    for j in range(early, column_count):
        inside(j)

    def carry_odd(j):
        chain_copy(j).wait_recv()
        relay_copy(j).start()
        carried = chain_in[j].astype(F32)
        moved = factor_in[j : j + 1, :] * carried

        @pl.when(plane < planes - 1)
        def _():
            chain_out[j] = (states[j] + factor_out[j : j + 1, :] * moved).astype(BF16)
            chain_copy(j).start()

        enter[j] = (pair_in[j].astype(F32) + moved).astype(BF16)

    def finish(j):
        offset, size, heads = columns[j]
        wide = j < wide_columns
        grown = spread([jnp.exp(running_columns[:, h : h + 1]) for h in heads])
        value = (base[j] + grown * dot(query_mix[...], enter[j])) * gate_act[j]
        square = value * value
        if len(heads) == 1:
            total = jnp.sum(square, axis=1, keepdims=True)
        else:
            first = jnp.sum(jnp.where(lane < NARROW_HEAD_DIM, square, 0.0), axis=1, keepdims=True)
            rest = jnp.sum(jnp.where(lane < NARROW_HEAD_DIM, 0.0, square), axis=1, keepdims=True)
            total = spread([first, rest])
        value = value * lax.rsqrt(total / (size // len(heads)) + NORM_EPS)
        gains = padded((wide_gain if wide else narrow_gain)[:, offset : offset + size])
        value = (value * gains).astype(BF16)
        start = offset if wide else wide_width + offset
        head_out[:, start : start + size] = value[:, :size]

    for j in range(column_count):

        @pl.when(jnp.logical_and(core == 1, plane > 0))
        def _():
            carry_odd(j)

        @pl.when(jnp.logical_and(core == 0, plane > 0))
        def _():
            relay_copy(j).wait_recv()
            enter[j] = chain_in[j]

        finish(j)

    loaded(16, 19)

    near = side - 1

    def first_copy(bundle, dim, k, other, d):
        part, in1, _, _, sems = bundle
        rows = in1.shape[4]
        if dim == 0:
            block = at((col + k) % side, (row + other) % side)
            peer = at((col + k) % side, row)
        else:
            block = at((col + other) % side, (row + k) % side)
            peer = at(col, (row + k) % side)
        return remote(
            part.at[d, block, pl.ds(dim * rows, rows)],
            in1.at[dim, k - 1, other, d],
            sems.at[0, d],
            sems.at[1 if other else 2, d],
            (me_s, peer),
        )

    def second_copy(bundle, dim, k, d):
        _, _, mid, in2, sems = bundle
        peer = at(col, (row + k) % side) if dim == 0 else at((col + k) % side, row)
        return remote(
            mid.at[dim, k - 1, d], in2.at[dim, k - 1, d], sems.at[3, d], sems.at[2, d], (me_s, peer)
        )

    def scatter(bundle, d, produce):
        part = bundle[0]
        shifts = [(a, b) for a in range(side) for b in range(side)]
        shifts.sort(key=lambda s: -((s[0] > 0) + (s[1] > 0)))
        for a, b in shifts:
            block = at((col + a) % side, (row + b) % side)
            part[d, block] = produce(block).astype(BF16)
            if a:
                first_copy(bundle, 0, a, b, d).start()
            if b:
                first_copy(bundle, 1, b, a, d).start()

    def forward(bundle, d):
        part, in1, mid, _, sems = bundle
        rows = in1.shape[4]
        spent(part.at[d, pl.ds(0, near * near)], sems.at[1, d])
        for k in peers:
            for dim in range(2):
                block = at(col, (row + k) % side) if dim == 0 else at((col + k) % side, row)
                total = part[d, block, dim * rows : (dim + 1) * rows].astype(F32)
                for j in peers:
                    total = total + in1[dim, j - 1, k, d].astype(F32)
                mid[dim, k - 1, d] = total.astype(BF16)
                second_copy(bundle, dim, k, d).start()

    def settle(bundle, d):
        spent(bundle[0].at[d, pl.ds(0, 2 * near)], bundle[4].at[2, d])

    def gathered(bundle, dim, d):
        part, in1, _, in2, _ = bundle
        rows = in1.shape[4]
        total = part[d, me_t, dim * rows : (dim + 1) * rows].astype(F32)
        for j in peers:
            total = total + in1[dim, j - 1, 0, d].astype(F32)
        for k in peers:
            total = total + in2[dim, k - 1, d].astype(F32)
        return total

    def sent(bundle, d):
        part, sems = bundle[0], bundle[4]
        spent(part.at[d, pl.ds(0, near * side)], sems.at[0, d])
        spent(part.at[d, pl.ds(0, near)], sems.at[3, d])

    def project(block):
        lanes = pl.ds(pl.multiple_of(block * width, LANES), width)
        return dot(head_out[...], head_rows_v[:, lanes])

    def spread_copy(buffer, sems, index, dim, k, d):
        part = buffer.at[me_t, d]
        peer = at((col + k) % side, row) if dim == 0 else at(col, (row + k) % side)
        return remote(part, part, sems.at[0, index], sems.at[1, index], (me_s, peer))

    def pass_copy(buffer, sems, index, dim, j, k, d):
        rows = buffer.shape[2] // 2
        if dim == 0:
            block = at((col + side - j) % side, row)
            peer = at(col, (row + k) % side)
        else:
            block = at(col, (row + side - j) % side)
            peer = at((col + k) % side, row)
        part = buffer.at[block, d, pl.ds(dim * rows, rows)]
        return remote(part, part, sems.at[2, index], sems.at[3, index], (me_s, peer))

    def spread_start(buffer, sems, d):
        for k in peers:
            for dim in range(2):
                spread_copy(buffer, sems, d, dim, k, d).start()

    def pass_start(buffer, sems, d):
        for dim in range(2):
            for j in peers:
                for k in peers:
                    pass_copy(buffer, sems, d, dim, j, k, d).start()

    def span(buffer, count, d):
        return buffer.at[pl.ds(0, count), d]

    heads_bundle = (head_part, head_in1, head_mid, head_in2, head_sems)
    sums_bundle = (partial, sum_in1, sum_mid, sum_in2, sum_sems)
    scatter(heads_bundle, 0, project)
    forward(heads_bundle, 0)
    settle(heads_bundle, 0)
    for dim in range(2):
        keep = slice(dim * half, (dim + 1) * half)
        value = gathered(heads_bundle, dim, 0) + resid_v[keep, :].astype(F32)
        hidden[keep, :] = value
        full[me_t, 0, keep, :] = value.astype(BF16)

    direct = sources == 1
    own = experts - 1
    ahead = 2
    far = own - min(FAR_GROUPS, own - 1)
    lag = 6
    own_slots = slice(own % sources * capacity, (own % sources + 1) * capacity)

    def pick(block, d):
        return dot(chooser[d], full[block, 0]).astype(BF16)

    def mate(d):
        mask = d + 1 + 2 * ((d + experts - 1) // experts)
        mask = mask - (experts - 2) * ((d + 3) // experts) - 4 * ((d + 1) // experts)
        where = me_s
        bit = 1
        while bit < experts:
            where = where + (mask // bit) % 2 * bit * (1 - 2 * ((me_s // bit) % 2))
            bit *= 2
        return where

    def slot(d):
        return pl.ds((d % sources) * capacity, capacity)

    def dispatch_copy(d):
        return remote(
            dispatch_out.at[d],
            tokens.at[me_t, d // sources, slot(d)],
            dispatch_send.at[0],
            dispatch_recv.at[d],
            (mate(d), me_t),
        )

    def partner_copy():
        return remote(
            partner_out,
            tokens.at[:, 0, pl.ds(0, capacity)],
            dispatch_send.at[1],
            dispatch_recv.at[0],
            (mate(0), me_t),
        )

    far_blocks = [at((col + j) % side, (row + k) % side) for j in peers for k in peers]

    def far_copy(n, d):
        return remote(
            far_out.at[n, d], tokens.at[far_blocks[n], d], far_send.at[0], far_recv.at[d], (mate(d), me_t)
        )

    def done_copy(d):
        return remote(
            done_out.at[d // sources, slot(d)],
            done_in.at[d],
            done_send.at[0],
            done_recv.at[d],
            (mate(d), me_t),
        )

    def send_dispatch(d, c):
        @pl.when(d < own)
        def _():
            dispatch_out[d] = pick(me_t, d)
            dispatch_copy(d).start()

        @pl.when(d == own)
        def _():
            tokens[me_t, groups - 1, own_slots] = pick(me_t, own)

        return c

    def send_far(d):
        for n, block in enumerate(far_blocks):
            far_out[n, d] = pick(block, d)
            far_copy(n, d).start()

    rows = tokens.shape[2] // 2

    def expert(d):
        pieces = [tokens[j, d].astype(F32) for j in range(shards)]
        square = jnp.zeros((2 * rows, 1), F32)
        for piece in pieces:
            square = square + jnp.sum(piece * piece, axis=1, keepdims=True)
        scale = lax.rsqrt(square / (shards * width) + NORM_EPS)
        normed = jnp.concatenate(
            [
                (piece * scale * gain_v[:, j * width : (j + 1) * width]).astype(BF16)
                for j, piece in enumerate(pieces)
            ],
            axis=1,
        )
        gate = dot(normed, gate_v[...])
        up = dot(normed, up_v[...])
        clamped = jnp.minimum(gate, CLAMP_LIMIT)
        act = (
            (jnp.clip(up, -CLAMP_LIMIT, CLAMP_LIMIT) + 1.0)
            * clamped
            * sigmoid(SIGMOID_SCALE * clamped)
        ).astype(BF16)

        def down(block):
            lanes = pl.ds(pl.multiple_of(block * width, LANES), width)
            return dot(act, down_v[:, lanes])

        scatter(sums_bundle, d, down)

    def combine(d, block):
        hidden[...] += dot(weight_high[d], block) + dot(weight_low[d], block)

    def between(value, low, high):
        return jnp.logical_and(value >= low, value < high)

    def take_done(d, c):
        done_copy(d).wait_recv()
        combine(d, done_in[d])
        return c

    def spread_wait(d):
        spent(span(tokens, 2 * near, d), token_sems.at[1, d])

    def pass_wait(d):
        spent(span(tokens, near * near, d), token_sems.at[3, d])

    def arrive_direct(i):
        dispatch_copy(i).wait_recv()
        spread_start(tokens, token_sems, i)

    late = plane >= planes // 2

    def feed_direct(i):
        @pl.when(jnp.logical_and(jnp.logical_not(late), between(i, 2, own)))
        def _():
            arrive_direct(i)

        @pl.when(i == 1)
        def _():
            spent(span(full, near * near, 0), early_sems.at[3, 0])
            for t in range(shards):
                partner_out[t] = pick(t, 0)
            partner_copy().start()

        @pl.when(jnp.logical_and(jnp.logical_not(late), i == 1))
        def _():
            arrive_direct(i)

        @pl.when(jnp.logical_and(late, between(i, 1, own - 1)))
        def _():
            arrive_direct(i + 1)

        @pl.when(between(i - 1, 1, far))
        def _():
            spread_wait(i - 1)
            pass_start(tokens, token_sems, i - 1)

    def launch_direct(i):
        @pl.when(between(i, 1, own - ahead))
        def _():
            send_dispatch(i + ahead, 0)

        @pl.when(between(i + ahead, far, own))
        def _():
            send_far(i + ahead)

        @pl.when(i == 2)
        def _():
            for t in range(shards):
                tokens[t, groups - 1] = pick(t, own)

    def ready_direct(d):
        @pl.when(d == 0)
        def _():
            partner_copy().wait_recv()

        @pl.when(between(d, 1, far))
        def _():
            pass_wait(d)

        @pl.when(between(d, far, own))
        def _():
            spread_wait(d)
            spent(far_out.at[:, d], far_recv.at[d])

    def feed_grouped(i):
        @pl.when(i < groups)
        def _():
            def arrive(d, c):
                @pl.when(d < own)
                def _():
                    dispatch_copy(d).wait_recv()

                return c

            lax.fori_loop(i * sources, (i + 1) * sources, arrive, 0)
            spread_start(tokens, token_sems, i)

        @pl.when(between(i - 1, 0, groups))
        def _():
            spread_wait(i - 1)
            pass_start(tokens, token_sems, i - 1)

        @pl.when(between(i, 1, groups - ahead))
        def _():
            launch(i + ahead)

    def launch(group):
        lax.fori_loop(group * sources, (group + 1) * sources, send_dispatch, 0)

    def early_sent():
        @pl.when(me_s < experts - 1)
        def _():
            for copy in rim_copies():
                copy.wait_send()

        @pl.when(core == 0)
        def _():
            pair_copy(column_count).wait_send()
            spent(state_out, pair_send.at[0])

        @pl.when(jnp.logical_and(core == 1, plane < planes - 1))
        def _():
            spent(chain_out, chain_send.at[0])

        @pl.when(jnp.logical_and(core == 1, plane > 0))
        def _():
            spent(chain_in, relay_send.at[0])

        sent(heads_bundle, 0)
        if direct:
            spent(span(full, 2 * near, 0), early_sems.at[0, 0])
            spent(span(full, near * near, 0), early_sems.at[2, 0])

    def tokens_sent(d):
        spent(span(tokens, 2 * near, d), token_sems.at[0, d])

    def passes_sent(d):
        spent(span(tokens, near * near, d), token_sems.at[2, d])

    steps = groups + 4

    def step(i, c):
        if direct:
            feed_direct(i)
        else:
            feed_grouped(i)

        @pl.when(between(i - 3, 0, groups))
        def _():
            forward(sums_bundle, i - 3)

        @pl.when(between(i - 2, 0, groups))
        def _():
            if direct:
                ready_direct(i - 2)
            else:
                pass_wait(i - 2)
            expert(i - 2)

        if direct:
            launch_direct(i)

        @pl.when(between(i - 4, 0, groups))
        def _():
            settle(sums_bundle, i - 4)
            for dim in range(2):
                done_out[i - 4, dim * rows : (dim + 1) * rows] = gathered(
                    sums_bundle, dim, i - 4
                ).astype(BF16)

            def leave(d, c):
                @pl.when(d < own)
                def _():
                    done_copy(d).start()

                return c

            lax.fori_loop((i - 4) * sources, (i - 3) * sources, leave, 0)

        @pl.when(between(i - lag, 0, groups))
        def _():
            lax.fori_loop((i - lag) * sources, (i - lag + 1) * sources, take_done, 0)
            sent(sums_bundle, i - lag)

        if direct:

            @pl.when(between(i - 4, 1, own))
            def _():
                tokens_sent(i - 4)

            @pl.when(between(i - 4, 1, far))
            def _():
                passes_sent(i - 4)
        else:

            @pl.when(between(i - 4, 0, groups))
            def _():
                tokens_sent(i - 4)
                passes_sent(i - 4)

        @pl.when(i == 3)
        def _():
            early_sent()

        return c

    if direct:
        spread_start(full, early_sems, 0)
        for d in range(1, min(ahead + 1, own)):
            send_dispatch(d, 0)
        loaded(19, 22)
        spent(span(full, 2 * near, 0), early_sems.at[1, 0])
        pass_start(full, early_sems, 0)

        @pl.when(late)
        def _():
            arrive_direct(1)
    else:
        for group in range(min(ahead + 1, groups)):
            launch(group)
        loaded(19, 22)
    lax.fori_loop(1 if direct else 0, steps, step, 0)
    lax.fori_loop((steps - lag) * sources, own, take_done, 0)
    combine(own, done_out[groups - 1, own_slots])
    out_v[...] = hidden[...].astype(BF16)
    out_copy = pltpu.make_async_copy(out_v, out_ref, load_sem.at[0])
    out_copy.start()
    if direct:
        spent(dispatch_out.at[pl.ds(1, own - 1)], dispatch_send.at[0])
        partner_copy().wait_send()
        if far < own:
            spent(far_out.at[:, pl.ds(0, own - far)], far_send.at[0])
    else:
        spent(dispatch_out.at[pl.ds(0, own)], dispatch_send.at[0])
    spent(done_in.at[pl.ds(0, own)], done_send.at[0])
    for group in range(steps - lag, groups):
        sent(sums_bundle, group)
    out_copy.wait()


def layer_call(side, experts, arrays):
    resid, narrow, wide, key = arrays[:4]
    step, decay = arrays[7], arrays[8]
    gate, up, down = arrays[22:]
    routes = arrays[20]
    length = resid.shape[0]
    shards = side * side
    width = resid.shape[1] // shards
    capacity = 4 * length * routes.shape[0] // (3 * experts)
    sources = max(1, min(experts, 128 // capacity))
    groups = experts // sources
    rows = sources * capacity
    state = key.shape[1] // GROUPS
    wide_width, narrow_width = wide.shape[1], narrow.shape[1]
    column_count = wide_width // LANES + -(-narrow_width // LANES)
    head_rows = wide_width + narrow_width
    near = side - 1
    tap_count = arrays[11].shape[0]
    vmem = pltpu.VMEM
    dma = pltpu.SemaphoreType.DMA
    scratch = [
        vmem((RIM, wide_width + 2 * state), BF16),
        vmem((RIM, narrow_width), BF16),
        vmem((RIM + length, wide_width + 2 * state), BF16),
        vmem((RIM + length, narrow_width), BF16),
        vmem((length, wide_width), BF16),
        vmem((length, narrow_width), BF16),
        vmem(step.shape, BF16),
        vmem(step.shape, F32),
        vmem((tap_count, narrow_width), F32),
        vmem((tap_count, wide_width), F32),
        vmem((tap_count, state), F32),
        vmem((tap_count, state), F32),
        vmem((1, narrow_width), F32),
        vmem((1, wide_width), F32),
        vmem((head_rows, resid.shape[1]), BF16),
        vmem((1, resid.shape[1]), F32),
        vmem(routes.shape, jnp.int32),
        vmem(routes.shape, F32),
        vmem((length, width), BF16),
        vmem(gate.shape[1:], BF16),
        vmem(up.shape[1:], BF16),
        vmem(down.shape[1:], BF16),
        vmem((8, length), F32),
        vmem((8, length), F32),
        vmem((column_count, length, LANES), F32),
        vmem((column_count, length, LANES), BF16),
        vmem((length, state), F32),
        vmem((length, state), BF16),
        vmem((length, length), F32),
        vmem((column_count, length, LANES), F32),
        vmem((column_count, length, LANES), F32),
        vmem((column_count, state, LANES), F32),
        vmem((column_count, state, LANES), BF16),
        vmem((column_count, state, LANES), BF16),
        vmem((column_count, state, LANES), BF16),
        vmem((column_count, state, LANES), BF16),
        vmem((column_count, state, LANES), BF16),
        vmem((8, LANES), F32),
        vmem((8, LANES), F32),
        vmem((length, head_rows), BF16),
        vmem((1, shards, length, width), BF16),
        vmem((2, near, side, 1, length // 2, width), BF16),
        vmem((2, near, 1, length // 2, width), BF16),
        vmem((2, near, 1, length // 2, width), BF16),
        vmem((length, width), F32),
        vmem((experts, capacity, length), BF16),
        vmem((experts, length, capacity), BF16),
        vmem((experts, length, capacity), BF16),
        vmem((experts, capacity, width), BF16),
        vmem((shards, groups, rows, width), BF16),
        vmem((groups, shards, rows, width), BF16),
        vmem((2, near, side, groups, rows // 2, width), BF16),
        vmem((2, near, groups, rows // 2, width), BF16),
        vmem((2, near, groups, rows // 2, width), BF16),
        vmem((groups, rows, width), BF16),
        vmem((experts, capacity, width), BF16),
        vmem((shards, 1, length, width), BF16),
        vmem((shards, capacity, width), BF16),
        vmem((near * near, groups, rows, width), BF16),
        vmem((length, width), BF16),
        dma((22,)),
        dma((2,)),
        dma((2,)),
        dma((2,)),
        dma((2,)),
        dma((1,)),
        dma((column_count,)),
        dma((1,)),
        dma((column_count,)),
        dma((4, 1)),
        dma((4, 1)),
        dma((2,)),
        dma((experts,)),
        dma((1,)),
        dma((groups,)),
        dma((4, groups)),
        dma((4, groups)),
        dma((1,)),
        dma((experts,)),
    ]
    hbm = pl.BlockSpec(memory_space=pl.ANY)
    smem = pl.BlockSpec(memory_space=pltpu.SMEM)
    specs = [hbm] * len(arrays)
    specs[8] = smem
    specs[10] = smem
    return pl.pallas_call(
        functools.partial(layer_kernel, side, experts, capacity),
        out_shape=jax.ShapeDtypeStruct((length, width), BF16),
        in_specs=specs,
        out_specs=hbm,
        scratch_shapes=scratch,
        compiler_params=pltpu.CompilerParams(
            collective_id=0, has_side_effects=True, vmem_limit_bytes=60 * 1024 * 1024
        ),
    )(*arrays)


def local(*arrays):
    arrays = list(arrays)
    shards = lax.axis_size("tp")
    side = int(round(shards**0.5))
    assert side * side == shards
    for i in (7, 9):
        arrays[i] = jnp.transpose(arrays[i], (1, 2, 0))
    for i in (15, 16, 19):
        arrays[i] = arrays[i][None, :]
    for i in (20, 21):
        arrays[i] = jnp.transpose(arrays[i])
    return layer_call(side, lax.axis_size("sp"), arrays)


def solution(mesh):
    return jax.shard_map(
        local,
        mesh=mesh,
        in_specs=(
            P("sp", None),
            P("sp", "tp"),
            P("sp", "tp"),
            P("sp", None),
            P("sp", None),
            P("sp", "tp"),
            P("sp", "tp"),
            P("sp", None, "tp"),
            P(None, "tp"),
            P("sp", None, "tp"),
            P(None, "tp"),
            P(None, "tp"),
            P(None, "tp"),
            P(),
            P(),
            P("tp"),
            P("tp"),
            P("tp", None),
            P("tp", None),
            P(),
            P("sp", None),
            P("sp", None),
            P("sp", None, "tp"),
            P("sp", None, "tp"),
            P("sp", "tp", None),
        ),
        out_specs=P("sp", "tp"),
        check_vma=False,
    )
```

```python
import functools

import jax
import jax.numpy as jnp
from jax import lax
from jax.experimental import pallas as pl
from jax.experimental.pallas import tpu as pltpu
from jax.sharding import PartitionSpec as P

HEADS = 16
NARROW_HEAD_DIM = 64
GROUPS = 4
LANES = 128
RIM = 16
FAR_GROUPS = 4

NORM_EPS = 1e-06
CLAMP_LIMIT = 7.0
SIGMOID_SCALE = 1.702

BF16, F32 = jnp.bfloat16, jnp.float32


def sigmoid(v):
    return 0.5 * jnp.tanh(0.5 * v) + 0.5


def dot(a, b):
    return jnp.dot(a, b, preferred_element_type=F32)


def layer_kernel(
    side,
    experts,
    capacity,
    resid_hbm,
    narrow_hbm,
    wide_hbm,
    key_hbm,
    query_hbm,
    narrow_gate_hbm,
    wide_gate_hbm,
    step_hbm,
    decay_ref,
    position_hbm,
    direct_ref,
    narrow_taps_hbm,
    wide_taps_hbm,
    key_taps_hbm,
    query_taps_hbm,
    narrow_gain_hbm,
    wide_gain_hbm,
    narrow_rows_hbm,
    wide_rows_hbm,
    gain_hbm,
    routes_hbm,
    route_weights_hbm,
    gate_hbm,
    up_hbm,
    down_hbm,
    out_ref,
    rim_wide,
    rim_narrow,
    wide_in,
    narrow_in,
    wide_gate_v,
    narrow_gate_v,
    step_v,
    position_v,
    narrow_taps,
    wide_taps,
    key_taps,
    query_taps,
    narrow_gain,
    wide_gain,
    head_rows_v,
    gain_v,
    routes_v,
    route_weights_v,
    resid_v,
    gate_v,
    up_v,
    down_v,
    step_rows,
    decay_rows,
    mix,
    mix_low,
    key_mix,
    query_mix,
    scores,
    base,
    gate_act,
    states,
    state_out,
    pair_in,
    chain_in,
    chain_out,
    enter,
    factor_out,
    factor_in,
    head_out,
    head_part,
    head_in1,
    head_mid,
    head_in2,
    hidden,
    chooser,
    weight_high,
    weight_low,
    dispatch_out,
    tokens,
    partial,
    sum_in1,
    sum_mid,
    sum_in2,
    done_out,
    done_in,
    full,
    partner_out,
    far_out,
    out_v,
    load_sem,
    rim_send,
    rim_recv,
    pair_send,
    pair_recv,
    chain_send,
    chain_recv,
    relay_send,
    relay_recv,
    head_sems,
    early_sems,
    dispatch_send,
    dispatch_recv,
    far_send,
    far_recv,
    token_sems,
    sum_sems,
    done_send,
    done_recv,
):
    me_s = lax.axis_index("sp")
    me_t = lax.axis_index("tp")
    col = me_t % side
    row = me_t // side
    core = me_s % 2
    plane = me_s // 2
    planes = experts // 2
    length, width = resid_v.shape
    shards = side * side
    groups = tokens.shape[1]
    sources = experts // groups
    state = key_hbm.shape[1] // GROUPS
    head_count = decay_ref.shape[1]
    wide_width = wide_hbm.shape[1]
    narrow_width = narrow_hbm.shape[1]
    peers = range(1, side)
    wide_columns = wide_width // LANES
    columns = []
    for i in range(wide_columns):
        columns.append((i * LANES, LANES, (head_count + i,)))
    for i in range(-(-narrow_width // LANES)):
        size = min(LANES, narrow_width - i * LANES)
        first = i * (LANES // NARROW_HEAD_DIM)
        columns.append(
            (i * LANES, size, tuple(first + k for k in range(size // NARROW_HEAD_DIM)))
        )
    column_count = len(columns)

    def at(c, r):
        return r * side + c

    def remote(src, dst, send, recv, where):
        return pltpu.make_async_remote_copy(
            src_ref=src,
            dst_ref=dst,
            send_sem=send,
            recv_sem=recv,
            device_id=where,
            device_id_type=pl.DeviceIdType.MESH,
        )

    group_column = pl.multiple_of(me_t * head_count // (HEADS // GROUPS) * state, LANES)
    own_columns = pl.ds(pl.multiple_of(me_t * width, LANES), width)
    group_slice = pl.ds(group_column, state)
    body = pl.ds(RIM, length)
    edge = pl.ds(length - RIM, RIM)
    wide_part = pl.ds(0, wide_width)
    key_part = pl.ds(wide_width, state)
    query_part = pl.ds(wide_width + state, state)
    moves = (
        (0, wide_hbm.at[edge], rim_wide.at[:, wide_part]),
        (0, key_hbm.at[edge, group_slice], rim_wide.at[:, key_part]),
        (0, query_hbm.at[edge, group_slice], rim_wide.at[:, query_part]),
        (1, narrow_hbm.at[edge], rim_narrow),
        (2, wide_hbm, wide_in.at[body, wide_part]),
        (2, key_hbm.at[:, group_slice], wide_in.at[body, key_part]),
        (2, query_hbm.at[:, group_slice], wide_in.at[body, query_part]),
        (3, narrow_hbm, narrow_in.at[body]),
        (4, wide_taps_hbm, wide_taps),
        (5, key_taps_hbm.at[:, group_slice], key_taps),
        (6, query_taps_hbm.at[:, group_slice], query_taps),
        (7, narrow_taps_hbm, narrow_taps),
        (8, step_hbm, step_v),
        (9, position_hbm, position_v),
        (10, wide_gate_hbm, wide_gate_v),
        (11, narrow_gate_hbm, narrow_gate_v),
        (12, narrow_gain_hbm, narrow_gain),
        (13, wide_gain_hbm, wide_gain),
        (14, routes_hbm, routes_v),
        (15, route_weights_hbm, route_weights_v),
        (16, wide_rows_hbm, head_rows_v.at[wide_part]),
        (16, narrow_rows_hbm, head_rows_v.at[pl.ds(wide_width, narrow_width)]),
        (17, resid_hbm.at[:, own_columns], resid_v),
        (18, gain_hbm, gain_v),
        (19, gate_hbm.at[0], gate_v),
        (20, up_hbm.at[0], up_v),
        (21, down_hbm.at[0], down_v),
    )
    whole = {0: rim_wide, 2: wide_in.at[body], 16: head_rows_v}

    def load(first, last):
        for i, source, target in moves:
            if first <= i < last:
                pltpu.make_async_copy(source, target, load_sem.at[i]).start()

    def spent(ref, sem):
        pltpu.make_async_copy(ref, ref, sem).wait()

    def loaded(first, last):
        for i in range(first, last):
            ref = whole.get(i, [m[2] for m in moves if m[0] == i][0])
            spent(ref, load_sem.at[i])

    barrier = pltpu.get_barrier_semaphore()

    def greet(s, t):
        pl.semaphore_signal(
            barrier, inc=1, device_id=(s, t), device_id_type=pl.DeviceIdType.MESH
        )

    def greet_sp(d, c):
        greet((me_s + d) % experts, me_t)
        return c

    load(0, 2)
    lax.fori_loop(1, experts, greet_sp, 0)
    for k in peers:
        greet(me_s, at((col + k) % side, row))
        greet(me_s, at(col, (row + k) % side))
    load(2, 16)
    loaded(0, 2)
    pl.semaphore_wait(barrier, experts - 1 + 2 * (side - 1))

    head = pl.ds(0, RIM)

    def rim_copies():
        where = (me_s + 1, me_t)
        return (
            remote(rim_wide, wide_in.at[head], rim_send.at[0], rim_recv.at[0], where),
            remote(rim_narrow, narrow_in.at[head], rim_send.at[1], rim_recv.at[1], where),
        )

    @pl.when(me_s < experts - 1)
    def _():
        for copy in rim_copies():
            copy.start()

    @pl.when(me_s == 0)
    def _():
        wide_in[:RIM, :] = jnp.zeros((RIM, wide_in.shape[1]), BF16)
        narrow_in[:RIM, :] = jnp.zeros((RIM, narrow_in.shape[1]), BF16)

    load(16, 22)
    loaded(2, 10)

    def padded(v):
        if v.shape[1] == LANES:
            return v
        return jnp.concatenate([v, jnp.zeros((v.shape[0], LANES - v.shape[1]), v.dtype)], axis=1)

    def conv(source, offset, size, taps, tap_offset, first, count):
        rows = padded(source[first : first + count + RIM, offset : offset + size]).astype(F32)
        weights = padded(taps[:, tap_offset : tap_offset + size])
        total = weights[-1:] * rows
        last = taps.shape[0] - 1
        for k in range(1, last + 1):
            total = total + weights[last - k : last - k + 1] * pltpu.roll(rows, k, 0)
        total = total[RIM:]
        return total * sigmoid(total)

    def convolve(first, count):
        keep = slice(first, first + count)
        key_mix[keep, :] = conv(wide_in, wide_width, state, key_taps, 0, first, count)
        query_mix[keep, :] = conv(
            wide_in, wide_width + state, state, query_taps, 0, first, count
        ).astype(BF16)
        for j, (offset, size, _) in enumerate(columns):
            wide = j < wide_columns
            value = conv(
                wide_in if wide else narrow_in,
                offset,
                size,
                wide_taps if wide else narrow_taps,
                offset,
                first,
                count,
            )
            mix[j, keep, :] = value
            mix_low[j, keep, :] = value.astype(BF16)

    convolve(RIM, length - RIM)

    lane = lax.broadcasted_iota(jnp.int32, (1, LANES), 1)

    def spread(parts):
        if len(parts) == 1:
            return parts[0]
        return jnp.where(lane < NARROW_HEAD_DIM, parts[0], parts[1])

    step_rows[...] = jnp.ones(step_rows.shape, F32)
    decay_rows[...] = jnp.zeros(decay_rows.shape, F32)
    head_index = lax.broadcasted_iota(jnp.int32, (head_count, length), 0)
    for g in range(2):
        raw = step_v[g].astype(F32)
        soft = jnp.maximum(raw, 0.0) + jnp.log(1.0 + jnp.exp(-jnp.abs(raw)))
        rate = jnp.zeros((head_count, length), F32)
        for h in range(head_count):
            rate = jnp.where(head_index == h, decay_ref[g, h], rate)
        keep = slice(g * head_count, (g + 1) * head_count)
        step_rows[keep, :] = soft
        decay_rows[keep, :] = position_v[g] - jnp.exp(rate) * soft
    line = lax.broadcasted_iota(jnp.int32, (length, length), 0)
    across = lax.broadcasted_iota(jnp.int32, (length, length), 1)
    upto = jnp.where(line <= across, 1.0, 0.0).astype(BF16)
    decays = decay_rows[...]
    high = decays.astype(BF16)
    middle = (decays - high.astype(F32)).astype(BF16)
    low = (decays - high.astype(F32) - middle.astype(F32)).astype(BF16)
    running = dot(high, upto) + (dot(middle, upto) + dot(low, upto))
    rows_kept = running.shape[0]
    total_decay = running[:, length - 1 : length]
    log_step = jnp.log(step_rows[...])
    offset_rows = running - log_step
    tail_rows = jnp.exp(total_decay - offset_rows)
    factors = jnp.exp(total_decay)
    running_columns = jnp.transpose(
        jnp.concatenate([running, jnp.zeros((LANES - rows_kept, length), F32)], axis=0)
    )
    factor_rows = []
    for _, _, heads in columns:
        parts = [jnp.broadcast_to(factors[h : h + 1, :], (1, LANES)) for h in heads]
        factor_rows.append(spread(parts))
    for j, value in enumerate(factor_rows):
        factor_out[j : j + 1, :] = value

    def tables():
        loaded(10, 16)

        for j, (offset, size, _) in enumerate(columns):
            source = wide_gate_v if j < wide_columns else narrow_gate_v
            value = padded(source[:, offset : offset + size]).astype(F32)
            gate_act[j] = value * sigmoid(value)

        order = lax.broadcasted_iota(jnp.int32, (experts, length), 0)
        mask = jnp.where(order < experts - 3, order + 3, order + 5 - experts)
        mask = jnp.where(order == 0, 1, jnp.where(order == experts - 1, 0, mask))
        named = mask ^ me_s
        member = jnp.zeros((experts, length), F32)
        weight_rows = jnp.zeros((experts, length), F32)
        for k in range(routes_v.shape[0]):
            hit = routes_v[k : k + 1, :] == named
            member = jnp.where(hit, 1.0, member)
            weight_rows = jnp.where(hit, route_weights_v[k : k + 1, :], weight_rows)
        before = jnp.where(line < across, 1.0, 0.0).astype(BF16)
        ranks = dot(member.astype(BF16), before)
        ranks = jnp.where(member > 0.5, ranks, -1.0)
        slots = lax.broadcasted_iota(jnp.int32, (capacity, length), 0).astype(F32)
        slot_lanes = lax.broadcasted_iota(jnp.int32, (length, capacity), 1).astype(F32)
        filler = [jnp.zeros((LANES - experts, length), F32)] if experts < LANES else []
        rank_columns = jnp.transpose(jnp.concatenate([ranks] + filler, axis=0))
        weight_columns = jnp.transpose(jnp.concatenate([weight_rows] + filler, axis=0))
        for d in range(experts):
            chooser[d] = jnp.where(slots == ranks[d : d + 1, :], 1.0, 0.0).astype(BF16)
            weights = jnp.where(
                slot_lanes == rank_columns[:, d : d + 1], weight_columns[:, d : d + 1], 0.0
            )
            rounded = weights.astype(BF16)
            weight_high[d] = rounded
            weight_low[d] = (weights - rounded.astype(F32)).astype(BF16)

    @pl.when(plane > 0)
    def _():
        tables()

    @pl.when(me_s > 0)
    def _():
        for copy in rim_copies():
            copy.wait_recv()

    convolve(0, RIM)

    key_turned = jnp.transpose(key_mix[...])
    for j, (_, _, heads) in enumerate(columns):
        parts = [
            dot((key_turned * tail_rows[h : h + 1, :]).astype(BF16), mix_low[j]) for h in heads
        ]
        states[j] = spread(parts)

    partner = me_s + 1 - 2 * core

    def pair_copy(j):
        if j == column_count:
            return remote(
                factor_out, factor_in, pair_send.at[1], pair_recv.at[1], (partner, me_t)
            )
        return remote(
            state_out.at[j], pair_in.at[j], pair_send.at[0], pair_recv.at[0], (partner, me_t)
        )

    @pl.when(core == 0)
    def _():
        pair_copy(column_count).start()
        for j in range(column_count):
            state_out[j] = states[j].astype(BF16)
            pair_copy(j).start()

    scores[...] = dot(query_mix[...], key_turned.astype(BF16))
    half = length // 2
    below = lax.broadcasted_iota(jnp.int32, (half, half), 0)
    beside = lax.broadcasted_iota(jnp.int32, (half, half), 1)
    causal = below >= beside

    def direct_row(heads):
        parts = []
        for h in heads:
            value = direct_ref[h // head_count, h % head_count]
            parts.append(jnp.full((1, LANES), value, F32))
        return spread(parts)

    def inside(j):
        heads = columns[j][2]
        parts = []
        for h in heads:
            up_to = running_columns[:, h : h + 1]
            since = offset_rows[h : h + 1, :]
            top = jnp.where(causal, up_to[:half] - since[:, :half], -1e30)
            left = up_to[half:] - since[:, :half]
            right = jnp.where(causal, up_to[half:] - since[:, half:], -1e30)
            upper = dot(
                (scores[:half, :half] * jnp.exp(top)).astype(BF16), mix_low[j, :half, :]
            )
            lower = dot(
                (scores[half:, :half] * jnp.exp(left)).astype(BF16), mix_low[j, :half, :]
            ) + dot((scores[half:, half:] * jnp.exp(right)).astype(BF16), mix_low[j, half:, :])
            parts.append((upper, lower))
        direct = direct_row(heads)
        base[j, :half, :] = spread([p[0] for p in parts]) + direct * mix[j, :half, :]
        base[j, half:, :] = spread([p[1] for p in parts]) + direct * mix[j, half:, :]

    early = min(2, column_count)
    for j in range(early):
        inside(j)

    def chain_copy(j):
        return remote(
            chain_out.at[j], chain_in.at[j], chain_send.at[0], chain_recv.at[j], (me_s + 2, me_t)
        )

    def relay_copy(j):
        return remote(
            chain_in.at[j], chain_in.at[j], relay_send.at[0], relay_recv.at[j], (me_s - 1, me_t)
        )

    @pl.when(core == 1)
    def _():
        pair_copy(column_count).wait_recv()
        spent(pair_in, pair_recv.at[0])
        for j in range(column_count):
            states[j] += factor_out[j : j + 1, :] * pair_in[j].astype(F32)

    @pl.when(jnp.logical_and(core == 1, plane == 0))
    def _():
        for j in range(column_count):
            if planes > 1:
                chain_out[j] = states[j].astype(BF16)
                chain_copy(j).start()
            enter[j] = pair_in[j]

    @pl.when(jnp.logical_and(core == 0, plane == 0))
    def _():
        enter[...] = jnp.zeros(enter.shape, BF16)

    for j in range(early, column_count):
        inside(j)

    @pl.when(plane == 0)
    def _():
        tables()

    def carry_odd(j):
        chain_copy(j).wait_recv()
        relay_copy(j).start()
        carried = chain_in[j].astype(F32)
        moved = factor_in[j : j + 1, :] * carried

        @pl.when(plane < planes - 1)
        def _():
            chain_out[j] = (states[j] + factor_out[j : j + 1, :] * moved).astype(BF16)
            chain_copy(j).start()

        enter[j] = (pair_in[j].astype(F32) + moved).astype(BF16)

    def finish(j):
        offset, size, heads = columns[j]
        wide = j < wide_columns
        grown = spread([jnp.exp(running_columns[:, h : h + 1]) for h in heads])
        value = (base[j] + grown * dot(query_mix[...], enter[j])) * gate_act[j]
        square = value * value
        if len(heads) == 1:
            total = jnp.sum(square, axis=1, keepdims=True)
        else:
            first = jnp.sum(jnp.where(lane < NARROW_HEAD_DIM, square, 0.0), axis=1, keepdims=True)
            rest = jnp.sum(jnp.where(lane < NARROW_HEAD_DIM, 0.0, square), axis=1, keepdims=True)
            total = spread([first, rest])
        value = value * lax.rsqrt(total / (size // len(heads)) + NORM_EPS)
        gains = padded((wide_gain if wide else narrow_gain)[:, offset : offset + size])
        value = (value * gains).astype(BF16)
        start = offset if wide else wide_width + offset
        head_out[:, start : start + size] = value[:, :size]

    for j in range(column_count):

        @pl.when(jnp.logical_and(core == 1, plane > 0))
        def _():
            carry_odd(j)

        @pl.when(jnp.logical_and(core == 0, plane > 0))
        def _():
            relay_copy(j).wait_recv()
            enter[j] = chain_in[j]

        finish(j)

    loaded(16, 19)

    near = side - 1

    def first_copy(bundle, dim, k, other, d):
        part, in1, _, _, sems = bundle
        rows = in1.shape[4]
        if dim == 0:
            block = at((col + k) % side, (row + other) % side)
            peer = at((col + k) % side, row)
        else:
            block = at((col + other) % side, (row + k) % side)
            peer = at(col, (row + k) % side)
        return remote(
            part.at[d, block, pl.ds(dim * rows, rows)],
            in1.at[dim, k - 1, other, d],
            sems.at[0, d],
            sems.at[1 if other else 2, d],
            (me_s, peer),
        )

    def second_copy(bundle, dim, k, d):
        _, _, mid, in2, sems = bundle
        peer = at(col, (row + k) % side) if dim == 0 else at((col + k) % side, row)
        return remote(
            mid.at[dim, k - 1, d], in2.at[dim, k - 1, d], sems.at[3, d], sems.at[2, d], (me_s, peer)
        )

    def scatter(bundle, d, produce):
        part = bundle[0]
        shifts = [(a, b) for a in range(side) for b in range(side)]
        shifts.sort(key=lambda s: -((s[0] > 0) + (s[1] > 0)))
        for a, b in shifts:
            block = at((col + a) % side, (row + b) % side)
            part[d, block] = produce(block).astype(BF16)
            if a:
                first_copy(bundle, 0, a, b, d).start()
            if b:
                first_copy(bundle, 1, b, a, d).start()

    def forward(bundle, d):
        part, in1, mid, _, sems = bundle
        rows = in1.shape[4]
        spent(part.at[d, pl.ds(0, near * near)], sems.at[1, d])
        for k in peers:
            for dim in range(2):
                block = at(col, (row + k) % side) if dim == 0 else at((col + k) % side, row)
                total = part[d, block, dim * rows : (dim + 1) * rows].astype(F32)
                for j in peers:
                    total = total + in1[dim, j - 1, k, d].astype(F32)
                mid[dim, k - 1, d] = total.astype(BF16)
                second_copy(bundle, dim, k, d).start()

    def settle(bundle, d):
        spent(bundle[0].at[d, pl.ds(0, 2 * near)], bundle[4].at[2, d])

    def gathered(bundle, dim, d):
        part, in1, _, in2, _ = bundle
        rows = in1.shape[4]
        total = part[d, me_t, dim * rows : (dim + 1) * rows].astype(F32)
        for j in peers:
            total = total + in1[dim, j - 1, 0, d].astype(F32)
        for k in peers:
            total = total + in2[dim, k - 1, d].astype(F32)
        return total

    def sent(bundle, d):
        part, sems = bundle[0], bundle[4]
        spent(part.at[d, pl.ds(0, near * side)], sems.at[0, d])
        spent(part.at[d, pl.ds(0, near)], sems.at[3, d])

    def project(block):
        lanes = pl.ds(pl.multiple_of(block * width, LANES), width)
        return dot(head_out[...], head_rows_v[:, lanes])

    def spread_copy(buffer, sems, index, dim, k, d):
        part = buffer.at[me_t, d]
        peer = at((col + k) % side, row) if dim == 0 else at(col, (row + k) % side)
        return remote(part, part, sems.at[0, index], sems.at[1, index], (me_s, peer))

    def pass_copy(buffer, sems, index, dim, j, k, d):
        rows = buffer.shape[2] // 2
        if dim == 0:
            block = at((col + side - j) % side, row)
            peer = at(col, (row + k) % side)
        else:
            block = at(col, (row + side - j) % side)
            peer = at((col + k) % side, row)
        part = buffer.at[block, d, pl.ds(dim * rows, rows)]
        return remote(part, part, sems.at[2, index], sems.at[3, index], (me_s, peer))

    def spread_start(buffer, sems, d):
        for k in peers:
            for dim in range(2):
                spread_copy(buffer, sems, d, dim, k, d).start()

    def pass_start(buffer, sems, d):
        for dim in range(2):
            for j in peers:
                for k in peers:
                    pass_copy(buffer, sems, d, dim, j, k, d).start()

    def span(buffer, count, d):
        return buffer.at[pl.ds(0, count), d]

    heads_bundle = (head_part, head_in1, head_mid, head_in2, head_sems)
    sums_bundle = (partial, sum_in1, sum_mid, sum_in2, sum_sems)
    scatter(heads_bundle, 0, project)
    forward(heads_bundle, 0)
    settle(heads_bundle, 0)
    for dim in range(2):
        keep = slice(dim * half, (dim + 1) * half)
        value = gathered(heads_bundle, dim, 0) + resid_v[keep, :].astype(F32)
        hidden[keep, :] = value
        full[me_t, 0, keep, :] = value.astype(BF16)

    direct = sources == 1
    own = experts - 1
    ahead = 2
    far = own - min(FAR_GROUPS, own - 1)
    lag = 6
    own_slots = slice(own % sources * capacity, (own % sources + 1) * capacity)

    def pick(block, d):
        return dot(chooser[d], full[block, 0]).astype(BF16)

    def mate(d):
        mask = d + 1 + 2 * ((d + experts - 1) // experts)
        mask = mask - (experts - 2) * ((d + 3) // experts) - 4 * ((d + 1) // experts)
        where = me_s
        bit = 1
        while bit < experts:
            where = where + (mask // bit) % 2 * bit * (1 - 2 * ((me_s // bit) % 2))
            bit *= 2
        return where

    def slot(d):
        return pl.ds((d % sources) * capacity, capacity)

    def dispatch_copy(d):
        return remote(
            dispatch_out.at[d],
            tokens.at[me_t, d // sources, slot(d)],
            dispatch_send.at[0],
            dispatch_recv.at[d],
            (mate(d), me_t),
        )

    def partner_copy():
        return remote(
            partner_out,
            tokens.at[:, 0, pl.ds(0, capacity)],
            dispatch_send.at[1],
            dispatch_recv.at[0],
            (mate(0), me_t),
        )

    far_blocks = [at((col + j) % side, (row + k) % side) for j in peers for k in peers]

    def far_copy(n, d):
        return remote(
            far_out.at[n, d], tokens.at[far_blocks[n], d], far_send.at[0], far_recv.at[d], (mate(d), me_t)
        )

    def done_copy(d):
        return remote(
            done_out.at[d // sources, slot(d)],
            done_in.at[d],
            done_send.at[0],
            done_recv.at[d],
            (mate(d), me_t),
        )

    def send_dispatch(d, c):
        @pl.when(d < own)
        def _():
            dispatch_out[d] = pick(me_t, d)
            dispatch_copy(d).start()

        @pl.when(d == own)
        def _():
            tokens[me_t, groups - 1, own_slots] = pick(me_t, own)

        return c

    def send_far(d):
        for n, block in enumerate(far_blocks):
            far_out[n, d] = pick(block, d)
            far_copy(n, d).start()

    rows = tokens.shape[2] // 2

    def expert(d):
        pieces = [tokens[j, d].astype(F32) for j in range(shards)]
        square = jnp.zeros((2 * rows, 1), F32)
        for piece in pieces:
            square = square + jnp.sum(piece * piece, axis=1, keepdims=True)
        scale = lax.rsqrt(square / (shards * width) + NORM_EPS)
        normed = jnp.concatenate(
            [
                (piece * scale * gain_v[:, j * width : (j + 1) * width]).astype(BF16)
                for j, piece in enumerate(pieces)
            ],
            axis=1,
        )
        gate = dot(normed, gate_v[...])
        up = dot(normed, up_v[...])
        clamped = jnp.minimum(gate, CLAMP_LIMIT)
        act = (
            (jnp.clip(up, -CLAMP_LIMIT, CLAMP_LIMIT) + 1.0)
            * clamped
            * sigmoid(SIGMOID_SCALE * clamped)
        ).astype(BF16)

        def down(block):
            lanes = pl.ds(pl.multiple_of(block * width, LANES), width)
            return dot(act, down_v[:, lanes])

        scatter(sums_bundle, d, down)

    def combine(d, block):
        hidden[...] += dot(weight_high[d], block) + dot(weight_low[d], block)

    def between(value, low, high):
        return jnp.logical_and(value >= low, value < high)

    def take_done(d, c):
        done_copy(d).wait_recv()
        combine(d, done_in[d])
        return c

    def spread_wait(d):
        spent(span(tokens, 2 * near, d), token_sems.at[1, d])

    def pass_wait(d):
        spent(span(tokens, near * near, d), token_sems.at[3, d])

    def arrive_direct(i):
        dispatch_copy(i).wait_recv()
        spread_start(tokens, token_sems, i)

    late = plane >= planes // 2

    def feed_direct(i):
        @pl.when(jnp.logical_and(jnp.logical_not(late), between(i, 2, own)))
        def _():
            arrive_direct(i)

        @pl.when(i == 1)
        def _():
            spent(span(full, near * near, 0), early_sems.at[3, 0])
            for t in range(shards):
                partner_out[t] = pick(t, 0)
            partner_copy().start()
            send_dispatch(1 + ahead, 0)

        @pl.when(jnp.logical_and(jnp.logical_not(late), i == 1))
        def _():
            arrive_direct(i)

        @pl.when(jnp.logical_and(late, between(i, 1, own - 1)))
        def _():
            arrive_direct(i + 1)

        @pl.when(between(i - 1, 1, far))
        def _():
            spread_wait(i - 1)
            pass_start(tokens, token_sems, i - 1)

    def launch_direct(i):
        @pl.when(between(i, 2, own - ahead))
        def _():
            send_dispatch(i + ahead, 0)

        @pl.when(between(i + 1, far, own))
        def _():
            send_far(i + 1)

        @pl.when(i == 2)
        def _():
            for t in range(shards):
                tokens[t, groups - 1] = pick(t, own)

    def ready_direct(d):
        @pl.when(d == 0)
        def _():
            partner_copy().wait_recv()

        @pl.when(between(d, 1, far))
        def _():
            pass_wait(d)

        @pl.when(between(d, far, own))
        def _():
            spread_wait(d)
            spent(far_out.at[:, d], far_recv.at[d])

    def feed_grouped(i):
        @pl.when(i < groups)
        def _():
            def arrive(d, c):
                @pl.when(d < own)
                def _():
                    dispatch_copy(d).wait_recv()

                return c

            lax.fori_loop(i * sources, (i + 1) * sources, arrive, 0)
            spread_start(tokens, token_sems, i)

        @pl.when(between(i - 1, 0, groups))
        def _():
            spread_wait(i - 1)
            pass_start(tokens, token_sems, i - 1)

        @pl.when(between(i, 1, groups - ahead))
        def _():
            launch(i + ahead)

    def launch(group):
        lax.fori_loop(group * sources, (group + 1) * sources, send_dispatch, 0)

    def early_sent():
        @pl.when(me_s < experts - 1)
        def _():
            for copy in rim_copies():
                copy.wait_send()

        @pl.when(core == 0)
        def _():
            pair_copy(column_count).wait_send()
            spent(state_out, pair_send.at[0])

        @pl.when(jnp.logical_and(core == 1, plane < planes - 1))
        def _():
            spent(chain_out, chain_send.at[0])

        @pl.when(jnp.logical_and(core == 1, plane > 0))
        def _():
            spent(chain_in, relay_send.at[0])

        sent(heads_bundle, 0)
        if direct:
            spent(span(full, 2 * near, 0), early_sems.at[0, 0])
            spent(span(full, near * near, 0), early_sems.at[2, 0])

    def tokens_sent(d):
        spent(span(tokens, 2 * near, d), token_sems.at[0, d])

    def passes_sent(d):
        spent(span(tokens, near * near, d), token_sems.at[2, d])

    steps = groups + 4

    def step(i, c):
        if direct:
            feed_direct(i)
        else:
            feed_grouped(i)

        @pl.when(between(i - 3, 0, groups))
        def _():
            forward(sums_bundle, i - 3)

        @pl.when(between(i - 2, 0, groups))
        def _():
            if direct:
                ready_direct(i - 2)
            else:
                pass_wait(i - 2)
            expert(i - 2)

        if direct:
            launch_direct(i)

        @pl.when(between(i - 4, 0, groups))
        def _():
            settle(sums_bundle, i - 4)
            for dim in range(2):
                done_out[i - 4, dim * rows : (dim + 1) * rows] = gathered(
                    sums_bundle, dim, i - 4
                ).astype(BF16)

            def leave(d, c):
                @pl.when(d < own)
                def _():
                    done_copy(d).start()

                return c

            lax.fori_loop((i - 4) * sources, (i - 3) * sources, leave, 0)

        @pl.when(between(i - lag, 0, groups))
        def _():
            lax.fori_loop((i - lag) * sources, (i - lag + 1) * sources, take_done, 0)
            sent(sums_bundle, i - lag)

        if direct:

            @pl.when(between(i - 4, 1, own))
            def _():
                tokens_sent(i - 4)

            @pl.when(between(i - 4, 1, far))
            def _():
                passes_sent(i - 4)
        else:

            @pl.when(between(i - 4, 0, groups))
            def _():
                tokens_sent(i - 4)
                passes_sent(i - 4)

        @pl.when(i == 3)
        def _():
            early_sent()

        return c

    if direct:
        spread_start(full, early_sems, 0)
        for d in range(1, min(ahead + 1, own)):
            send_dispatch(d, 0)
        loaded(19, 22)
        spent(span(full, 2 * near, 0), early_sems.at[1, 0])
        pass_start(full, early_sems, 0)

        @pl.when(late)
        def _():
            arrive_direct(1)
    else:
        for group in range(min(ahead + 1, groups)):
            launch(group)
        loaded(19, 22)
    lax.fori_loop(1 if direct else 0, steps, step, 0)
    lax.fori_loop((steps - lag) * sources, own, take_done, 0)
    combine(own, done_out[groups - 1, own_slots])
    out_v[...] = hidden[...].astype(BF16)
    out_copy = pltpu.make_async_copy(out_v, out_ref, load_sem.at[0])
    out_copy.start()
    if direct:
        spent(dispatch_out.at[pl.ds(1, own - 1)], dispatch_send.at[0])
        partner_copy().wait_send()
        if far < own:
            spent(far_out.at[:, pl.ds(0, own - far)], far_send.at[0])
    else:
        spent(dispatch_out.at[pl.ds(0, own)], dispatch_send.at[0])
    spent(done_in.at[pl.ds(0, own)], done_send.at[0])
    for group in range(steps - lag, groups):
        sent(sums_bundle, group)
    out_copy.wait()


def layer_call(side, experts, arrays):
    resid, narrow, wide, key = arrays[:4]
    step, decay = arrays[7], arrays[8]
    gate, up, down = arrays[22:]
    routes = arrays[20]
    length = resid.shape[0]
    shards = side * side
    width = resid.shape[1] // shards
    capacity = 4 * length * routes.shape[0] // (3 * experts)
    sources = max(1, min(experts, 128 // capacity))
    groups = experts // sources
    rows = sources * capacity
    state = key.shape[1] // GROUPS
    wide_width, narrow_width = wide.shape[1], narrow.shape[1]
    column_count = wide_width // LANES + -(-narrow_width // LANES)
    head_rows = wide_width + narrow_width
    near = side - 1
    tap_count = arrays[11].shape[0]
    vmem = pltpu.VMEM
    dma = pltpu.SemaphoreType.DMA
    scratch = [
        vmem((RIM, wide_width + 2 * state), BF16),
        vmem((RIM, narrow_width), BF16),
        vmem((RIM + length, wide_width + 2 * state), BF16),
        vmem((RIM + length, narrow_width), BF16),
        vmem((length, wide_width), BF16),
        vmem((length, narrow_width), BF16),
        vmem(step.shape, BF16),
        vmem(step.shape, F32),
        vmem((tap_count, narrow_width), F32),
        vmem((tap_count, wide_width), F32),
        vmem((tap_count, state), F32),
        vmem((tap_count, state), F32),
        vmem((1, narrow_width), F32),
        vmem((1, wide_width), F32),
        vmem((head_rows, resid.shape[1]), BF16),
        vmem((1, resid.shape[1]), F32),
        vmem(routes.shape, jnp.int32),
        vmem(routes.shape, F32),
        vmem((length, width), BF16),
        vmem(gate.shape[1:], BF16),
        vmem(up.shape[1:], BF16),
        vmem(down.shape[1:], BF16),
        vmem((8, length), F32),
        vmem((8, length), F32),
        vmem((column_count, length, LANES), F32),
        vmem((column_count, length, LANES), BF16),
        vmem((length, state), F32),
        vmem((length, state), BF16),
        vmem((length, length), F32),
        vmem((column_count, length, LANES), F32),
        vmem((column_count, length, LANES), F32),
        vmem((column_count, state, LANES), F32),
        vmem((column_count, state, LANES), BF16),
        vmem((column_count, state, LANES), BF16),
        vmem((column_count, state, LANES), BF16),
        vmem((column_count, state, LANES), BF16),
        vmem((column_count, state, LANES), BF16),
        vmem((8, LANES), F32),
        vmem((8, LANES), F32),
        vmem((length, head_rows), BF16),
        vmem((1, shards, length, width), BF16),
        vmem((2, near, side, 1, length // 2, width), BF16),
        vmem((2, near, 1, length // 2, width), BF16),
        vmem((2, near, 1, length // 2, width), BF16),
        vmem((length, width), F32),
        vmem((experts, capacity, length), BF16),
        vmem((experts, length, capacity), BF16),
        vmem((experts, length, capacity), BF16),
        vmem((experts, capacity, width), BF16),
        vmem((shards, groups, rows, width), BF16),
        vmem((groups, shards, rows, width), BF16),
        vmem((2, near, side, groups, rows // 2, width), BF16),
        vmem((2, near, groups, rows // 2, width), BF16),
        vmem((2, near, groups, rows // 2, width), BF16),
        vmem((groups, rows, width), BF16),
        vmem((experts, capacity, width), BF16),
        vmem((shards, 1, length, width), BF16),
        vmem((shards, capacity, width), BF16),
        vmem((near * near, groups, rows, width), BF16),
        vmem((length, width), BF16),
        dma((22,)),
        dma((2,)),
        dma((2,)),
        dma((2,)),
        dma((2,)),
        dma((1,)),
        dma((column_count,)),
        dma((1,)),
        dma((column_count,)),
        dma((4, 1)),
        dma((4, 1)),
        dma((2,)),
        dma((experts,)),
        dma((1,)),
        dma((groups,)),
        dma((4, groups)),
        dma((4, groups)),
        dma((1,)),
        dma((experts,)),
    ]
    hbm = pl.BlockSpec(memory_space=pl.ANY)
    smem = pl.BlockSpec(memory_space=pltpu.SMEM)
    specs = [hbm] * len(arrays)
    specs[8] = smem
    specs[10] = smem
    return pl.pallas_call(
        functools.partial(layer_kernel, side, experts, capacity),
        out_shape=jax.ShapeDtypeStruct((length, width), BF16),
        in_specs=specs,
        out_specs=hbm,
        scratch_shapes=scratch,
        compiler_params=pltpu.CompilerParams(
            collective_id=0, has_side_effects=True, vmem_limit_bytes=60 * 1024 * 1024
        ),
    )(*arrays)


def local(*arrays):
    arrays = list(arrays)
    shards = lax.axis_size("tp")
    side = int(round(shards**0.5))
    assert side * side == shards
    for i in (7, 9):
        arrays[i] = jnp.transpose(arrays[i], (1, 2, 0))
    for i in (15, 16, 19):
        arrays[i] = arrays[i][None, :]
    for i in (20, 21):
        arrays[i] = jnp.transpose(arrays[i])
    return layer_call(side, lax.axis_size("sp"), arrays)


def solution(mesh):
    return jax.shard_map(
        local,
        mesh=mesh,
        in_specs=(
            P("sp", None),
            P("sp", "tp"),
            P("sp", "tp"),
            P("sp", None),
            P("sp", None),
            P("sp", "tp"),
            P("sp", "tp"),
            P("sp", None, "tp"),
            P(None, "tp"),
            P("sp", None, "tp"),
            P(None, "tp"),
            P(None, "tp"),
            P(None, "tp"),
            P(),
            P(),
            P("tp"),
            P("tp"),
            P("tp", None),
            P("tp", None),
            P(),
            P("sp", None),
            P("sp", None),
            P("sp", None, "tp"),
            P("sp", None, "tp"),
            P("sp", "tp", None),
        ),
        out_specs=P("sp", "tp"),
        check_vma=False,
    )
```

```python
import functools

import jax
import jax.numpy as jnp
from jax import lax
from jax.experimental import pallas as pl
from jax.experimental.pallas import tpu as pltpu
from jax.sharding import PartitionSpec as P

HEADS = 16
NARROW_HEAD_DIM = 64
GROUPS = 4
LANES = 128
RIM = 16
FAR_GROUPS = 4

NORM_EPS = 1e-06
CLAMP_LIMIT = 7.0
SIGMOID_SCALE = 1.702

BF16, F32 = jnp.bfloat16, jnp.float32


def sigmoid(v):
    return 0.5 * jnp.tanh(0.5 * v) + 0.5


def dot(a, b):
    return jnp.dot(a, b, preferred_element_type=F32)


def layer_kernel(
    side,
    experts,
    capacity,
    resid_hbm,
    narrow_hbm,
    wide_hbm,
    key_hbm,
    query_hbm,
    narrow_gate_hbm,
    wide_gate_hbm,
    step_hbm,
    decay_ref,
    position_hbm,
    direct_ref,
    narrow_taps_hbm,
    wide_taps_hbm,
    key_taps_hbm,
    query_taps_hbm,
    narrow_gain_hbm,
    wide_gain_hbm,
    narrow_rows_hbm,
    wide_rows_hbm,
    gain_hbm,
    routes_hbm,
    route_weights_hbm,
    gate_hbm,
    up_hbm,
    down_hbm,
    out_ref,
    rim_wide,
    rim_narrow,
    wide_in,
    narrow_in,
    wide_gate_v,
    narrow_gate_v,
    step_v,
    position_v,
    narrow_taps,
    wide_taps,
    key_taps,
    query_taps,
    narrow_gain,
    wide_gain,
    head_rows_v,
    gain_v,
    routes_v,
    route_weights_v,
    resid_v,
    gate_v,
    up_v,
    down_v,
    step_rows,
    decay_rows,
    mix,
    mix_low,
    key_mix,
    query_mix,
    scores,
    base,
    gate_act,
    states,
    state_out,
    pair_in,
    chain_in,
    chain_out,
    enter,
    factor_out,
    factor_in,
    head_out,
    head_part,
    head_in1,
    head_mid,
    head_in2,
    hidden,
    chooser,
    weight_high,
    weight_low,
    dispatch_out,
    tokens,
    partial,
    sum_in1,
    sum_mid,
    sum_in2,
    done_out,
    done_in,
    full,
    partner_out,
    far_out,
    out_v,
    load_sem,
    rim_send,
    rim_recv,
    pair_send,
    pair_recv,
    chain_send,
    chain_recv,
    relay_send,
    relay_recv,
    head_sems,
    early_sems,
    dispatch_send,
    dispatch_recv,
    far_send,
    far_recv,
    token_sems,
    sum_sems,
    done_send,
    done_recv,
):
    me_s = lax.axis_index("sp")
    me_t = lax.axis_index("tp")
    col = me_t % side
    row = me_t // side
    core = me_s % 2
    plane = me_s // 2
    planes = experts // 2
    length, width = resid_v.shape
    shards = side * side
    groups = tokens.shape[1]
    sources = experts // groups
    state = key_hbm.shape[1] // GROUPS
    head_count = decay_ref.shape[1]
    wide_width = wide_hbm.shape[1]
    narrow_width = narrow_hbm.shape[1]
    peers = range(1, side)
    wide_columns = wide_width // LANES
    columns = []
    for i in range(wide_columns):
        columns.append((i * LANES, LANES, (head_count + i,)))
    for i in range(-(-narrow_width // LANES)):
        size = min(LANES, narrow_width - i * LANES)
        first = i * (LANES // NARROW_HEAD_DIM)
        columns.append(
            (i * LANES, size, tuple(first + k for k in range(size // NARROW_HEAD_DIM)))
        )
    column_count = len(columns)

    def at(c, r):
        return r * side + c

    def remote(src, dst, send, recv, where):
        return pltpu.make_async_remote_copy(
            src_ref=src,
            dst_ref=dst,
            send_sem=send,
            recv_sem=recv,
            device_id=where,
            device_id_type=pl.DeviceIdType.MESH,
        )

    group_column = pl.multiple_of(me_t * head_count // (HEADS // GROUPS) * state, LANES)
    own_columns = pl.ds(pl.multiple_of(me_t * width, LANES), width)
    group_slice = pl.ds(group_column, state)
    body = pl.ds(RIM, length)
    edge = pl.ds(length - RIM, RIM)
    wide_part = pl.ds(0, wide_width)
    key_part = pl.ds(wide_width, state)
    query_part = pl.ds(wide_width + state, state)
    moves = (
        (0, wide_hbm.at[edge], rim_wide.at[:, wide_part]),
        (0, key_hbm.at[edge, group_slice], rim_wide.at[:, key_part]),
        (0, query_hbm.at[edge, group_slice], rim_wide.at[:, query_part]),
        (1, narrow_hbm.at[edge], rim_narrow),
        (2, wide_hbm, wide_in.at[body, wide_part]),
        (2, key_hbm.at[:, group_slice], wide_in.at[body, key_part]),
        (2, query_hbm.at[:, group_slice], wide_in.at[body, query_part]),
        (3, narrow_hbm, narrow_in.at[body]),
        (4, wide_taps_hbm, wide_taps),
        (5, key_taps_hbm.at[:, group_slice], key_taps),
        (6, query_taps_hbm.at[:, group_slice], query_taps),
        (7, narrow_taps_hbm, narrow_taps),
        (8, step_hbm, step_v),
        (9, position_hbm, position_v),
        (10, wide_gate_hbm, wide_gate_v),
        (11, narrow_gate_hbm, narrow_gate_v),
        (12, narrow_gain_hbm, narrow_gain),
        (13, wide_gain_hbm, wide_gain),
        (14, routes_hbm, routes_v),
        (15, route_weights_hbm, route_weights_v),
        (16, wide_rows_hbm, head_rows_v.at[wide_part]),
        (16, narrow_rows_hbm, head_rows_v.at[pl.ds(wide_width, narrow_width)]),
        (17, resid_hbm.at[:, own_columns], resid_v),
        (18, gain_hbm, gain_v),
        (19, gate_hbm.at[0], gate_v),
        (20, up_hbm.at[0], up_v),
        (21, down_hbm.at[0], down_v),
    )
    whole = {0: rim_wide, 2: wide_in.at[body], 16: head_rows_v}

    def load(first, last):
        for i, source, target in moves:
            if first <= i < last:
                pltpu.make_async_copy(source, target, load_sem.at[i]).start()

    def spent(ref, sem):
        pltpu.make_async_copy(ref, ref, sem).wait()

    def loaded(first, last):
        for i in range(first, last):
            ref = whole.get(i, [m[2] for m in moves if m[0] == i][0])
            spent(ref, load_sem.at[i])

    barrier = pltpu.get_barrier_semaphore()

    def greet(s, t):
        pl.semaphore_signal(
            barrier, inc=1, device_id=(s, t), device_id_type=pl.DeviceIdType.MESH
        )

    def greet_sp(d, c):
        greet((me_s + d) % experts, me_t)
        return c

    load(0, 2)
    lax.fori_loop(1, experts, greet_sp, 0)
    for k in peers:
        greet(me_s, at((col + k) % side, row))
        greet(me_s, at(col, (row + k) % side))
    load(2, 16)
    loaded(0, 2)
    pl.semaphore_wait(barrier, experts - 1 + 2 * (side - 1))

    head = pl.ds(0, RIM)

    def rim_copies():
        where = (me_s + 1, me_t)
        return (
            remote(rim_wide, wide_in.at[head], rim_send.at[0], rim_recv.at[0], where),
            remote(rim_narrow, narrow_in.at[head], rim_send.at[1], rim_recv.at[1], where),
        )

    @pl.when(me_s < experts - 1)
    def _():
        for copy in rim_copies():
            copy.start()

    @pl.when(me_s == 0)
    def _():
        wide_in[:RIM, :] = jnp.zeros((RIM, wide_in.shape[1]), BF16)
        narrow_in[:RIM, :] = jnp.zeros((RIM, narrow_in.shape[1]), BF16)

    load(16, 22)
    loaded(2, 10)

    def padded(v):
        if v.shape[1] == LANES:
            return v
        return jnp.concatenate([v, jnp.zeros((v.shape[0], LANES - v.shape[1]), v.dtype)], axis=1)

    def conv(source, offset, size, taps, tap_offset, first, count):
        rows = padded(source[first : first + count + RIM, offset : offset + size]).astype(F32)
        weights = padded(taps[:, tap_offset : tap_offset + size])
        total = weights[-1:] * rows
        last = taps.shape[0] - 1
        for k in range(1, last + 1):
            total = total + weights[last - k : last - k + 1] * pltpu.roll(rows, k, 0)
        total = total[RIM:]
        return total * sigmoid(total)

    def convolve(first, count):
        keep = slice(first, first + count)
        key_mix[keep, :] = conv(wide_in, wide_width, state, key_taps, 0, first, count)
        query_mix[keep, :] = conv(
            wide_in, wide_width + state, state, query_taps, 0, first, count
        ).astype(BF16)
        for j, (offset, size, _) in enumerate(columns):
            wide = j < wide_columns
            value = conv(
                wide_in if wide else narrow_in,
                offset,
                size,
                wide_taps if wide else narrow_taps,
                offset,
                first,
                count,
            )
            mix[j, keep, :] = value
            mix_low[j, keep, :] = value.astype(BF16)

    convolve(RIM, length - RIM)

    lane = lax.broadcasted_iota(jnp.int32, (1, LANES), 1)

    def spread(parts):
        if len(parts) == 1:
            return parts[0]
        return jnp.where(lane < NARROW_HEAD_DIM, parts[0], parts[1])

    step_rows[...] = jnp.ones(step_rows.shape, F32)
    decay_rows[...] = jnp.zeros(decay_rows.shape, F32)
    head_index = lax.broadcasted_iota(jnp.int32, (head_count, length), 0)
    for g in range(2):
        raw = step_v[g].astype(F32)
        soft = jnp.maximum(raw, 0.0) + jnp.log(1.0 + jnp.exp(-jnp.abs(raw)))
        rate = jnp.zeros((head_count, length), F32)
        for h in range(head_count):
            rate = jnp.where(head_index == h, decay_ref[g, h], rate)
        keep = slice(g * head_count, (g + 1) * head_count)
        step_rows[keep, :] = soft
        decay_rows[keep, :] = position_v[g] - jnp.exp(rate) * soft
    line = lax.broadcasted_iota(jnp.int32, (length, length), 0)
    across = lax.broadcasted_iota(jnp.int32, (length, length), 1)
    upto = jnp.where(line <= across, 1.0, 0.0).astype(BF16)
    decays = decay_rows[...]
    high = decays.astype(BF16)
    middle = (decays - high.astype(F32)).astype(BF16)
    low = (decays - high.astype(F32) - middle.astype(F32)).astype(BF16)
    running = dot(high, upto) + (dot(middle, upto) + dot(low, upto))
    rows_kept = running.shape[0]
    total_decay = running[:, length - 1 : length]
    log_step = jnp.log(step_rows[...])
    offset_rows = running - log_step
    tail_rows = jnp.exp(total_decay - offset_rows)
    factors = jnp.exp(total_decay)
    running_columns = jnp.transpose(
        jnp.concatenate([running, jnp.zeros((LANES - rows_kept, length), F32)], axis=0)
    )
    factor_rows = []
    for _, _, heads in columns:
        parts = [jnp.broadcast_to(factors[h : h + 1, :], (1, LANES)) for h in heads]
        factor_rows.append(spread(parts))
    for j, value in enumerate(factor_rows):
        factor_out[j : j + 1, :] = value

    def tables():
        loaded(10, 16)

        for j, (offset, size, _) in enumerate(columns):
            source = wide_gate_v if j < wide_columns else narrow_gate_v
            value = padded(source[:, offset : offset + size]).astype(F32)
            gate_act[j] = value * sigmoid(value)

        order = lax.broadcasted_iota(jnp.int32, (experts, length), 0)
        mask = jnp.where(order < experts - 3, order + 3, order + 5 - experts)
        mask = jnp.where(order == 0, 1, jnp.where(order == experts - 1, 0, mask))
        named = mask ^ me_s
        member = jnp.zeros((experts, length), F32)
        weight_rows = jnp.zeros((experts, length), F32)
        for k in range(routes_v.shape[0]):
            hit = routes_v[k : k + 1, :] == named
            member = jnp.where(hit, 1.0, member)
            weight_rows = jnp.where(hit, route_weights_v[k : k + 1, :], weight_rows)
        before = jnp.where(line < across, 1.0, 0.0).astype(BF16)
        ranks = dot(member.astype(BF16), before)
        ranks = jnp.where(member > 0.5, ranks, -1.0)
        slots = lax.broadcasted_iota(jnp.int32, (capacity, length), 0).astype(F32)
        slot_lanes = lax.broadcasted_iota(jnp.int32, (length, capacity), 1).astype(F32)
        filler = [jnp.zeros((LANES - experts, length), F32)] if experts < LANES else []
        rank_columns = jnp.transpose(jnp.concatenate([ranks] + filler, axis=0))
        weight_columns = jnp.transpose(jnp.concatenate([weight_rows] + filler, axis=0))
        for d in range(experts):
            chooser[d] = jnp.where(slots == ranks[d : d + 1, :], 1.0, 0.0).astype(BF16)
            weights = jnp.where(
                slot_lanes == rank_columns[:, d : d + 1], weight_columns[:, d : d + 1], 0.0
            )
            rounded = weights.astype(BF16)
            weight_high[d] = rounded
            weight_low[d] = (weights - rounded.astype(F32)).astype(BF16)

    @pl.when(plane > 0)
    def _():
        tables()

    @pl.when(me_s > 0)
    def _():
        for copy in rim_copies():
            copy.wait_recv()

    convolve(0, RIM)

    key_turned = jnp.transpose(key_mix[...])
    for j, (_, _, heads) in enumerate(columns):
        parts = [
            dot((key_turned * tail_rows[h : h + 1, :]).astype(BF16), mix_low[j]) for h in heads
        ]
        states[j] = spread(parts)

    partner = me_s + 1 - 2 * core

    def pair_copy(j):
        if j == column_count:
            return remote(
                factor_out, factor_in, pair_send.at[1], pair_recv.at[1], (partner, me_t)
            )
        return remote(
            state_out.at[j], pair_in.at[j], pair_send.at[0], pair_recv.at[0], (partner, me_t)
        )

    @pl.when(core == 0)
    def _():
        pair_copy(column_count).start()
        for j in range(column_count):
            state_out[j] = states[j].astype(BF16)
            pair_copy(j).start()

    scores[...] = dot(query_mix[...], key_turned.astype(BF16))
    half = length // 2
    below = lax.broadcasted_iota(jnp.int32, (half, half), 0)
    beside = lax.broadcasted_iota(jnp.int32, (half, half), 1)
    causal = below >= beside

    def direct_row(heads):
        parts = []
        for h in heads:
            value = direct_ref[h // head_count, h % head_count]
            parts.append(jnp.full((1, LANES), value, F32))
        return spread(parts)

    def inside(j):
        heads = columns[j][2]
        parts = []
        for h in heads:
            up_to = running_columns[:, h : h + 1]
            since = offset_rows[h : h + 1, :]
            top = jnp.where(causal, up_to[:half] - since[:, :half], -1e30)
            left = up_to[half:] - since[:, :half]
            right = jnp.where(causal, up_to[half:] - since[:, half:], -1e30)
            upper = dot(
                (scores[:half, :half] * jnp.exp(top)).astype(BF16), mix_low[j, :half, :]
            )
            lower = dot(
                (scores[half:, :half] * jnp.exp(left)).astype(BF16), mix_low[j, :half, :]
            ) + dot((scores[half:, half:] * jnp.exp(right)).astype(BF16), mix_low[j, half:, :])
            parts.append((upper, lower))
        direct = direct_row(heads)
        base[j, :half, :] = spread([p[0] for p in parts]) + direct * mix[j, :half, :]
        base[j, half:, :] = spread([p[1] for p in parts]) + direct * mix[j, half:, :]

    early = min(2, column_count)
    for j in range(early):
        inside(j)

    def chain_copy(j):
        return remote(
            chain_out.at[j], chain_in.at[j], chain_send.at[0], chain_recv.at[j], (me_s + 2, me_t)
        )

    def relay_copy(j):
        return remote(
            chain_in.at[j], chain_in.at[j], relay_send.at[0], relay_recv.at[j], (me_s - 1, me_t)
        )

    @pl.when(core == 1)
    def _():
        pair_copy(column_count).wait_recv()
        spent(pair_in, pair_recv.at[0])
        for j in range(column_count):
            states[j] += factor_out[j : j + 1, :] * pair_in[j].astype(F32)

    @pl.when(jnp.logical_and(core == 1, plane == 0))
    def _():
        for j in range(column_count):
            if planes > 1:
                chain_out[j] = states[j].astype(BF16)
                chain_copy(j).start()
            enter[j] = pair_in[j]

    @pl.when(jnp.logical_and(core == 0, plane == 0))
    def _():
        enter[...] = jnp.zeros(enter.shape, BF16)

    for j in range(early, column_count):
        inside(j)

    @pl.when(plane == 0)
    def _():
        tables()

    def carry_odd(j):
        chain_copy(j).wait_recv()
        relay_copy(j).start()
        carried = chain_in[j].astype(F32)
        moved = factor_in[j : j + 1, :] * carried

        @pl.when(plane < planes - 1)
        def _():
            chain_out[j] = (states[j] + factor_out[j : j + 1, :] * moved).astype(BF16)
            chain_copy(j).start()

        enter[j] = (pair_in[j].astype(F32) + moved).astype(BF16)

    def finish(j):
        offset, size, heads = columns[j]
        wide = j < wide_columns
        grown = spread([jnp.exp(running_columns[:, h : h + 1]) for h in heads])
        value = (base[j] + grown * dot(query_mix[...], enter[j])) * gate_act[j]
        square = value * value
        if len(heads) == 1:
            total = jnp.sum(square, axis=1, keepdims=True)
        else:
            first = jnp.sum(jnp.where(lane < NARROW_HEAD_DIM, square, 0.0), axis=1, keepdims=True)
            rest = jnp.sum(jnp.where(lane < NARROW_HEAD_DIM, 0.0, square), axis=1, keepdims=True)
            total = spread([first, rest])
        value = value * lax.rsqrt(total / (size // len(heads)) + NORM_EPS)
        gains = padded((wide_gain if wide else narrow_gain)[:, offset : offset + size])
        value = (value * gains).astype(BF16)
        start = offset if wide else wide_width + offset
        head_out[:, start : start + size] = value[:, :size]

    for j in range(column_count):

        @pl.when(jnp.logical_and(core == 1, plane > 0))
        def _():
            carry_odd(j)

        @pl.when(jnp.logical_and(core == 0, plane > 0))
        def _():
            relay_copy(j).wait_recv()
            enter[j] = chain_in[j]

        finish(j)

    loaded(16, 19)

    near = side - 1

    def first_copy(bundle, dim, k, other, d):
        part, in1, _, _, sems = bundle
        rows = in1.shape[4]
        if dim == 0:
            block = at((col + k) % side, (row + other) % side)
            peer = at((col + k) % side, row)
        else:
            block = at((col + other) % side, (row + k) % side)
            peer = at(col, (row + k) % side)
        return remote(
            part.at[d, block, pl.ds(dim * rows, rows)],
            in1.at[dim, k - 1, other, d],
            sems.at[0, d],
            sems.at[1 if other else 2, d],
            (me_s, peer),
        )

    def second_copy(bundle, dim, k, d):
        _, _, mid, in2, sems = bundle
        peer = at(col, (row + k) % side) if dim == 0 else at((col + k) % side, row)
        return remote(
            mid.at[dim, k - 1, d], in2.at[dim, k - 1, d], sems.at[0, d], sems.at[2, d], (me_s, peer)
        )

    def scatter(bundle, d, produce):
        part = bundle[0]
        shifts = [(a, b) for a in range(side) for b in range(side)]
        shifts.sort(key=lambda s: -((s[0] > 0) + (s[1] > 0)))
        for a, b in shifts:
            block = at((col + a) % side, (row + b) % side)
            part[d, block] = produce(block).astype(BF16)
            if a:
                first_copy(bundle, 0, a, b, d).start()
            if b:
                first_copy(bundle, 1, b, a, d).start()

    def forward(bundle, d):
        part, in1, mid, _, sems = bundle
        rows = in1.shape[4]
        spent(part.at[d, pl.ds(0, near * near)], sems.at[1, d])
        for k in peers:
            for dim in range(2):
                block = at(col, (row + k) % side) if dim == 0 else at((col + k) % side, row)
                total = part[d, block, dim * rows : (dim + 1) * rows].astype(F32)
                for j in peers:
                    total = total + in1[dim, j - 1, k, d].astype(F32)
                mid[dim, k - 1, d] = total.astype(BF16)
                second_copy(bundle, dim, k, d).start()

    def settle(bundle, d):
        spent(bundle[0].at[d, pl.ds(0, 2 * near)], bundle[4].at[2, d])

    def gathered(bundle, dim, d):
        part, in1, _, in2, _ = bundle
        rows = in1.shape[4]
        total = part[d, me_t, dim * rows : (dim + 1) * rows].astype(F32)
        for j in peers:
            total = total + in1[dim, j - 1, 0, d].astype(F32)
        for k in peers:
            total = total + in2[dim, k - 1, d].astype(F32)
        return total

    def sent(bundle, d):
        part, sems = bundle[0], bundle[4]
        spent(part.at[d, pl.ds(0, near * side + near)], sems.at[0, d])

    def project(block):
        lanes = pl.ds(pl.multiple_of(block * width, LANES), width)
        return dot(head_out[...], head_rows_v[:, lanes])

    def spread_copy(buffer, sems, index, dim, k, d):
        part = buffer.at[me_t, d]
        peer = at((col + k) % side, row) if dim == 0 else at(col, (row + k) % side)
        return remote(part, part, sems.at[0, index], sems.at[1, index], (me_s, peer))

    def pass_copy(buffer, sems, index, dim, j, k, d):
        rows = buffer.shape[2] // 2
        if dim == 0:
            block = at((col + side - j) % side, row)
            peer = at(col, (row + k) % side)
        else:
            block = at(col, (row + side - j) % side)
            peer = at((col + k) % side, row)
        part = buffer.at[block, d, pl.ds(dim * rows, rows)]
        return remote(part, part, sems.at[2, index], sems.at[3, index], (me_s, peer))

    def spread_start(buffer, sems, d):
        for k in peers:
            for dim in range(2):
                spread_copy(buffer, sems, d, dim, k, d).start()

    def pass_start(buffer, sems, d):
        for dim in range(2):
            for j in peers:
                for k in peers:
                    pass_copy(buffer, sems, d, dim, j, k, d).start()

    def span(buffer, count, d):
        return buffer.at[pl.ds(0, count), d]

    heads_bundle = (head_part, head_in1, head_mid, head_in2, head_sems)
    sums_bundle = (partial, sum_in1, sum_mid, sum_in2, sum_sems)
    scatter(heads_bundle, 0, project)
    forward(heads_bundle, 0)
    settle(heads_bundle, 0)
    for dim in range(2):
        keep = slice(dim * half, (dim + 1) * half)
        value = gathered(heads_bundle, dim, 0) + resid_v[keep, :].astype(F32)
        hidden[keep, :] = value
        full[me_t, 0, keep, :] = value.astype(BF16)

    direct = sources == 1
    own = experts - 1
    ahead = 2
    far = own - min(FAR_GROUPS, own - 1)
    lag = 6
    own_slots = slice(own % sources * capacity, (own % sources + 1) * capacity)

    def pick(block, d):
        return dot(chooser[d], full[block, 0]).astype(BF16)

    def mate(d):
        mask = d + 1 + 2 * ((d + experts - 1) // experts)
        mask = mask - (experts - 2) * ((d + 3) // experts) - 4 * ((d + 1) // experts)
        where = me_s
        bit = 1
        while bit < experts:
            where = where + (mask // bit) % 2 * bit * (1 - 2 * ((me_s // bit) % 2))
            bit *= 2
        return where

    def slot(d):
        return pl.ds((d % sources) * capacity, capacity)

    def dispatch_copy(d):
        return remote(
            dispatch_out.at[d],
            tokens.at[me_t, d // sources, slot(d)],
            dispatch_send.at[0],
            dispatch_recv.at[d],
            (mate(d), me_t),
        )

    def partner_copy():
        return remote(
            partner_out,
            tokens.at[:, 0, pl.ds(0, capacity)],
            dispatch_send.at[1],
            dispatch_recv.at[0],
            (mate(0), me_t),
        )

    far_blocks = [at((col + j) % side, (row + k) % side) for j in peers for k in peers]

    def far_copy(n, d):
        return remote(
            far_out.at[n, d], tokens.at[far_blocks[n], d], far_send.at[0], far_recv.at[d], (mate(d), me_t)
        )

    def done_copy(d):
        return remote(
            done_out.at[d // sources, slot(d)],
            done_in.at[d],
            done_send.at[0],
            done_recv.at[d],
            (mate(d), me_t),
        )

    def send_dispatch(d, c):
        @pl.when(d < own)
        def _():
            dispatch_out[d] = pick(me_t, d)
            dispatch_copy(d).start()

        @pl.when(d == own)
        def _():
            tokens[me_t, groups - 1, own_slots] = pick(me_t, own)

        return c

    def send_far(d):
        for n, block in enumerate(far_blocks):
            far_out[n, d] = pick(block, d)
            far_copy(n, d).start()

    rows = tokens.shape[2] // 2

    def expert(d):
        pieces = [tokens[j, d].astype(F32) for j in range(shards)]
        square = jnp.zeros((2 * rows, 1), F32)
        for piece in pieces:
            square = square + jnp.sum(piece * piece, axis=1, keepdims=True)
        scale = lax.rsqrt(square / (shards * width) + NORM_EPS)
        normed = jnp.concatenate(
            [
                (piece * scale * gain_v[:, j * width : (j + 1) * width]).astype(BF16)
                for j, piece in enumerate(pieces)
            ],
            axis=1,
        )
        gate = dot(normed, gate_v[...])
        up = dot(normed, up_v[...])
        clamped = jnp.minimum(gate, CLAMP_LIMIT)
        act = (
            (jnp.clip(up, -CLAMP_LIMIT, CLAMP_LIMIT) + 1.0)
            * clamped
            * sigmoid(SIGMOID_SCALE * clamped)
        ).astype(BF16)

        def down(block):
            lanes = pl.ds(pl.multiple_of(block * width, LANES), width)
            return dot(act, down_v[:, lanes])

        scatter(sums_bundle, d, down)

    def combine(d, block):
        hidden[...] += dot(weight_high[d], block) + dot(weight_low[d], block)

    def between(value, low, high):
        return jnp.logical_and(value >= low, value < high)

    def take_done(d, c):
        done_copy(d).wait_recv()
        combine(d, done_in[d])
        return c

    def spread_wait(d):
        spent(span(tokens, 2 * near, d), token_sems.at[1, d])

    def pass_wait(d):
        spent(span(tokens, near * near, d), token_sems.at[3, d])

    def arrive_direct(i):
        dispatch_copy(i).wait_recv()
        spread_start(tokens, token_sems, i)

    late = plane >= planes // 2

    def feed_direct(i):
        @pl.when(jnp.logical_and(jnp.logical_not(late), between(i, 2, own)))
        def _():
            arrive_direct(i)

        @pl.when(i == 1)
        def _():
            spent(span(full, near * near, 0), early_sems.at[3, 0])
            for t in range(shards):
                partner_out[t] = pick(t, 0)
            partner_copy().start()
            send_dispatch(1 + ahead, 0)

        @pl.when(jnp.logical_and(jnp.logical_not(late), i == 1))
        def _():
            arrive_direct(i)

        @pl.when(jnp.logical_and(late, between(i, 1, own - 1)))
        def _():
            arrive_direct(i + 1)

        @pl.when(between(i - 1, 1, far))
        def _():
            spread_wait(i - 1)
            pass_start(tokens, token_sems, i - 1)

    def launch_direct(i):
        @pl.when(between(i, 2, own - ahead))
        def _():
            send_dispatch(i + ahead, 0)

        @pl.when(between(i + 1, far, own))
        def _():
            send_far(i + 1)

        @pl.when(i == 2)
        def _():
            for t in range(shards):
                tokens[t, groups - 1] = pick(t, own)

    def ready_direct(d):
        @pl.when(d == 0)
        def _():
            partner_copy().wait_recv()

        @pl.when(between(d, 1, far))
        def _():
            pass_wait(d)

        @pl.when(between(d, far, own))
        def _():
            spread_wait(d)
            spent(far_out.at[:, d], far_recv.at[d])

    def feed_grouped(i):
        @pl.when(i < groups)
        def _():
            def arrive(d, c):
                @pl.when(d < own)
                def _():
                    dispatch_copy(d).wait_recv()

                return c

            lax.fori_loop(i * sources, (i + 1) * sources, arrive, 0)
            spread_start(tokens, token_sems, i)

        @pl.when(between(i - 1, 0, groups))
        def _():
            spread_wait(i - 1)
            pass_start(tokens, token_sems, i - 1)

        @pl.when(between(i, 1, groups - ahead))
        def _():
            launch(i + ahead)

    def launch(group):
        lax.fori_loop(group * sources, (group + 1) * sources, send_dispatch, 0)

    def early_sent():
        @pl.when(me_s < experts - 1)
        def _():
            for copy in rim_copies():
                copy.wait_send()

        @pl.when(core == 0)
        def _():
            pair_copy(column_count).wait_send()
            spent(state_out, pair_send.at[0])

        @pl.when(jnp.logical_and(core == 1, plane < planes - 1))
        def _():
            spent(chain_out, chain_send.at[0])

        @pl.when(jnp.logical_and(core == 1, plane > 0))
        def _():
            spent(chain_in, relay_send.at[0])

        sent(heads_bundle, 0)
        if direct:
            spent(span(full, 2 * near, 0), early_sems.at[0, 0])
            spent(span(full, near * near, 0), early_sems.at[2, 0])

    def tokens_sent(d):
        spent(span(tokens, 2 * near, d), token_sems.at[0, d])

    def passes_sent(d):
        spent(span(tokens, near * near, d), token_sems.at[2, d])

    steps = groups + 4

    def step(i, c):
        if direct:
            feed_direct(i)
        else:
            feed_grouped(i)

        @pl.when(between(i - 3, 0, groups))
        def _():
            forward(sums_bundle, i - 3)

        @pl.when(between(i - 2, 0, groups))
        def _():
            if direct:
                ready_direct(i - 2)
            else:
                pass_wait(i - 2)
            expert(i - 2)

        if direct:
            launch_direct(i)

        @pl.when(between(i - 4, 0, groups))
        def _():
            settle(sums_bundle, i - 4)
            for dim in range(2):
                done_out[i - 4, dim * rows : (dim + 1) * rows] = gathered(
                    sums_bundle, dim, i - 4
                ).astype(BF16)

            def leave(d, c):
                @pl.when(d < own)
                def _():
                    done_copy(d).start()

                return c

            lax.fori_loop((i - 4) * sources, (i - 3) * sources, leave, 0)

        @pl.when(between(i - lag, 0, groups))
        def _():
            lax.fori_loop((i - lag) * sources, (i - lag + 1) * sources, take_done, 0)
            sent(sums_bundle, i - lag)

        if direct:

            @pl.when(between(i - 4, 1, own))
            def _():
                tokens_sent(i - 4)

            @pl.when(between(i - 4, 1, far))
            def _():
                passes_sent(i - 4)
        else:

            @pl.when(between(i - 4, 0, groups))
            def _():
                tokens_sent(i - 4)
                passes_sent(i - 4)

        @pl.when(i == 3)
        def _():
            early_sent()

        return c

    if direct:
        spread_start(full, early_sems, 0)
        for d in range(1, min(ahead + 1, own)):
            send_dispatch(d, 0)
        loaded(19, 22)
        spent(span(full, 2 * near, 0), early_sems.at[1, 0])
        pass_start(full, early_sems, 0)

        @pl.when(late)
        def _():
            arrive_direct(1)
    else:
        for group in range(min(ahead + 1, groups)):
            launch(group)
        loaded(19, 22)
    lax.fori_loop(1 if direct else 0, steps, step, 0)
    lax.fori_loop((steps - lag) * sources, own, take_done, 0)
    combine(own, done_out[groups - 1, own_slots])
    out_v[...] = hidden[...].astype(BF16)
    out_copy = pltpu.make_async_copy(out_v, out_ref, load_sem.at[0])
    out_copy.start()
    if direct:
        spent(dispatch_out.at[pl.ds(1, own - 1)], dispatch_send.at[0])
        partner_copy().wait_send()
        if far < own:
            spent(far_out.at[:, pl.ds(0, own - far)], far_send.at[0])
    else:
        spent(dispatch_out.at[pl.ds(0, own)], dispatch_send.at[0])
    spent(done_in.at[pl.ds(0, own)], done_send.at[0])
    for group in range(steps - lag, groups):
        sent(sums_bundle, group)
    out_copy.wait()


def layer_call(side, experts, arrays):
    resid, narrow, wide, key = arrays[:4]
    step, decay = arrays[7], arrays[8]
    gate, up, down = arrays[22:]
    routes = arrays[20]
    length = resid.shape[0]
    shards = side * side
    width = resid.shape[1] // shards
    capacity = 4 * length * routes.shape[0] // (3 * experts)
    sources = max(1, min(experts, 128 // capacity))
    groups = experts // sources
    rows = sources * capacity
    state = key.shape[1] // GROUPS
    wide_width, narrow_width = wide.shape[1], narrow.shape[1]
    column_count = wide_width // LANES + -(-narrow_width // LANES)
    head_rows = wide_width + narrow_width
    near = side - 1
    tap_count = arrays[11].shape[0]
    vmem = pltpu.VMEM
    dma = pltpu.SemaphoreType.DMA
    scratch = [
        vmem((RIM, wide_width + 2 * state), BF16),
        vmem((RIM, narrow_width), BF16),
        vmem((RIM + length, wide_width + 2 * state), BF16),
        vmem((RIM + length, narrow_width), BF16),
        vmem((length, wide_width), BF16),
        vmem((length, narrow_width), BF16),
        vmem(step.shape, BF16),
        vmem(step.shape, F32),
        vmem((tap_count, narrow_width), F32),
        vmem((tap_count, wide_width), F32),
        vmem((tap_count, state), F32),
        vmem((tap_count, state), F32),
        vmem((1, narrow_width), F32),
        vmem((1, wide_width), F32),
        vmem((head_rows, resid.shape[1]), BF16),
        vmem((1, resid.shape[1]), F32),
        vmem(routes.shape, jnp.int32),
        vmem(routes.shape, F32),
        vmem((length, width), BF16),
        vmem(gate.shape[1:], BF16),
        vmem(up.shape[1:], BF16),
        vmem(down.shape[1:], BF16),
        vmem((8, length), F32),
        vmem((8, length), F32),
        vmem((column_count, length, LANES), F32),
        vmem((column_count, length, LANES), BF16),
        vmem((length, state), F32),
        vmem((length, state), BF16),
        vmem((length, length), F32),
        vmem((column_count, length, LANES), F32),
        vmem((column_count, length, LANES), F32),
        vmem((column_count, state, LANES), F32),
        vmem((column_count, state, LANES), BF16),
        vmem((column_count, state, LANES), BF16),
        vmem((column_count, state, LANES), BF16),
        vmem((column_count, state, LANES), BF16),
        vmem((column_count, state, LANES), BF16),
        vmem((8, LANES), F32),
        vmem((8, LANES), F32),
        vmem((length, head_rows), BF16),
        vmem((1, shards, length, width), BF16),
        vmem((2, near, side, 1, length // 2, width), BF16),
        vmem((2, near, 1, length // 2, width), BF16),
        vmem((2, near, 1, length // 2, width), BF16),
        vmem((length, width), F32),
        vmem((experts, capacity, length), BF16),
        vmem((experts, length, capacity), BF16),
        vmem((experts, length, capacity), BF16),
        vmem((experts, capacity, width), BF16),
        vmem((shards, groups, rows, width), BF16),
        vmem((groups, shards, rows, width), BF16),
        vmem((2, near, side, groups, rows // 2, width), BF16),
        vmem((2, near, groups, rows // 2, width), BF16),
        vmem((2, near, groups, rows // 2, width), BF16),
        vmem((groups, rows, width), BF16),
        vmem((experts, capacity, width), BF16),
        vmem((shards, 1, length, width), BF16),
        vmem((shards, capacity, width), BF16),
        vmem((near * near, groups, rows, width), BF16),
        vmem((length, width), BF16),
        dma((22,)),
        dma((2,)),
        dma((2,)),
        dma((2,)),
        dma((2,)),
        dma((1,)),
        dma((column_count,)),
        dma((1,)),
        dma((column_count,)),
        dma((3, 1)),
        dma((4, 1)),
        dma((2,)),
        dma((experts,)),
        dma((1,)),
        dma((groups,)),
        dma((4, groups)),
        dma((3, groups)),
        dma((1,)),
        dma((experts,)),
    ]
    hbm = pl.BlockSpec(memory_space=pl.ANY)
    smem = pl.BlockSpec(memory_space=pltpu.SMEM)
    specs = [hbm] * len(arrays)
    specs[8] = smem
    specs[10] = smem
    return pl.pallas_call(
        functools.partial(layer_kernel, side, experts, capacity),
        out_shape=jax.ShapeDtypeStruct((length, width), BF16),
        in_specs=specs,
        out_specs=hbm,
        scratch_shapes=scratch,
        compiler_params=pltpu.CompilerParams(
            collective_id=0, has_side_effects=True, vmem_limit_bytes=60 * 1024 * 1024
        ),
    )(*arrays)


def local(*arrays):
    arrays = list(arrays)
    shards = lax.axis_size("tp")
    side = int(round(shards**0.5))
    assert side * side == shards
    for i in (7, 9):
        arrays[i] = jnp.transpose(arrays[i], (1, 2, 0))
    for i in (15, 16, 19):
        arrays[i] = arrays[i][None, :]
    for i in (20, 21):
        arrays[i] = jnp.transpose(arrays[i])
    return layer_call(side, lax.axis_size("sp"), arrays)


def solution(mesh):
    return jax.shard_map(
        local,
        mesh=mesh,
        in_specs=(
            P("sp", None),
            P("sp", "tp"),
            P("sp", "tp"),
            P("sp", None),
            P("sp", None),
            P("sp", "tp"),
            P("sp", "tp"),
            P("sp", None, "tp"),
            P(None, "tp"),
            P("sp", None, "tp"),
            P(None, "tp"),
            P(None, "tp"),
            P(None, "tp"),
            P(),
            P(),
            P("tp"),
            P("tp"),
            P("tp", None),
            P("tp", None),
            P(),
            P("sp", None),
            P("sp", None),
            P("sp", None, "tp"),
            P("sp", None, "tp"),
            P("sp", "tp", None),
        ),
        out_specs=P("sp", "tp"),
        check_vma=False,
    )
```
